32 devices in a mesh: grp: 2 (over y), sp: 4 (over z), tp: 4 (over x, core).
Axes of the slice: x: 2, y: 2, z: 4, core: 2. Of those that a mesh axis runs over, the one named last changes fastest.
Arguments:
- tokens: bfloat16 [4096, 2048], P(('grp', 'sp')), parts along dimension 0, may hold values from -6 to 6
- gate_in: bfloat16 [2, 2048, 512], P(None, 'sp', 'tp'), may hold values from -0.125 to 0.125
- gate_conv: bfloat16 [2, 2048, 512], P(None, 'sp', 'tp'), may hold values from -0.125 to 0.125
- value_in: bfloat16 [2, 2048, 512], P(None, 'sp', 'tp'), may hold values from -0.125 to 0.125
- out_weight: bfloat16 [2, 512, 2048], P(None, None, 'sp'), may hold values from -0.25 to 0.25
- conv_taps: float32 [2, 3, 512], replicated, may hold values from -7 to 7
- pre_gain: float32 [2, 2048], replicated, may hold values from 0.1 to 1.9
- mix_gain: float32 [2, 512], replicated, may hold values from 0.1 to 1.9
- post_gain: float32 [2, 2048], replicated, may hold values from 0.1 to 1.9
Outputs:
- result: bfloat16 [4096, 2048], P(('grp', 'sp', 'tp')), parts along dimension 0
The draws below stay inside these ranges and needn't reach their ends.
There are 2 independent parts, one for each index of `grp`. The reference program is written for one: setup_inputs(seed, part) draws one part's arguments, and reference() takes and returns one part's arrays. A program takes and returns all parts, laid end to end along the dimension named above; an argument that names none is the same for every part. Nothing has to cross between parts.
All inputs are finite; a program needn't handle non-finite values.
Results may differ from the reference program's by a relative error of at most 0.011.
Values may be sent and summed in bfloat16 or wider, within the bound.
A program may use at most 64 MiB of HBM per device.

```python
import math
import jax
import jax.numpy as jnp
from jax import lax

D = 2048
S = 512
TAPS = 3
LAYERS = 2
TOKENS = 2048
TP_CH = 128


def draw_conv_taps(key, part):
    first_key, second_key = jax.random.split(jax.random.fold_in(key, 11))
    blocks = S // TP_CH
    orders = jax.vmap(lambda one_key: jax.random.permutation(one_key, blocks))(jax.random.split(first_key, LAYERS))
    ladder = 0.3 * jnp.power(10.0, orders.astype(jnp.float32) / max(blocks - 1, 1))
    raw_taps = jnp.clip(jax.random.normal(second_key, (LAYERS, TAPS, S), jnp.float32), -4.0, 4.0)
    scales = jnp.repeat(ladder, TP_CH, axis=1)
    return raw_taps * scales[:, None, :] / math.sqrt(TAPS)


def shard_levels(key, shape, shards, smallest, top_value):
    level = 1.0
    for dim, shards_of in shards:
        heights = jax.random.uniform(jax.random.fold_in(jax.random.fold_in(key, 6), dim), (shards_of,), jnp.float32, smallest / len(shards), top_value / len(shards))
        level = level * jnp.repeat(jnp.exp(heights), shape[dim] // shards_of).reshape((-1,) + (1,) * (len(shape) - 1 - dim))
    return level


def scatter_about(own_key, extent, scale, limit, cuts=(), dtype=jnp.bfloat16):
    loudness = shard_levels(own_key, extent, cuts, -0.22, 0.18) if cuts else 1.0
    array = jax.random.normal(own_key, extent, jnp.float32) * scale * loudness
    return jnp.minimum(jnp.maximum(array, -limit), limit).astype(dtype)


def setup_inputs(seed: int = 0, part: int = 0) -> dict:
    splits = jax.random.split(jax.random.key(seed), 10)
    own_keys = jax.random.split(jax.random.fold_in(splits[9], part), 10)
    return {
        "tokens": scatter_about(own_keys[0], (TOKENS, D), 1.0, 6.0, ((0, 4),)),
        "gate_in": scatter_about(splits[1], (LAYERS, D, S), D ** -0.5, 0.125, ((1, 4), (2, 4))),
        "gate_conv": scatter_about(splits[2], (LAYERS, D, S), D ** -0.5, 0.125, ((1, 4), (2, 4))),
        "value_in": scatter_about(splits[3], (LAYERS, D, S), D ** -0.5, 0.125, ((1, 4), (2, 4))),
        "out_weight": scatter_about(splits[4], (LAYERS, S, D), S ** -0.5, 0.25, ((2, 4),)),
        "conv_taps": draw_conv_taps(jax.random.fold_in(splits[9], 71), part),
        "pre_gain": jnp.clip(1.0 + 0.18 * jax.random.normal(splits[6], (LAYERS, D), jnp.float32), 0.1, 1.9),
        "mix_gain": jnp.clip(1.0 + 0.18 * jax.random.normal(splits[7], (LAYERS, S), jnp.float32), 0.1, 1.9),
        "post_gain": jnp.clip(1.0 + 0.18 * jax.random.normal(splits[8], (LAYERS, D), jnp.float32), 0.1, 1.9),
    }


EPS = 1e-06

def rms_norm(values, gain):
    return values * lax.rsqrt(lax.optimization_barrier(jnp.mean(values * values, axis=-1, keepdims=True)) + EPS) * gain

def stored(values):
    return lax.optimization_barrier(values.astype(jnp.bfloat16))

def reference(tokens, gate_in, gate_conv, value_in, out_weight, conv_taps, pre_gain, mix_gain, post_gain):
    stream = tokens.astype(jnp.float32)
    for layer_index in range(LAYERS):
        normed = stored(rms_norm(stream, pre_gain[layer_index]))
        outer = stored(jnp.dot(normed, gate_in[layer_index], preferred_element_type=jnp.float32))
        inner = stored(jnp.dot(normed, gate_conv[layer_index], preferred_element_type=jnp.float32))
        values = stored(jnp.dot(normed, value_in[layer_index], preferred_element_type=jnp.float32))
        gated = stored(inner.astype(jnp.float32) * values.astype(jnp.float32))
        padded = jnp.concatenate([jnp.zeros((TAPS - 1, S), jnp.bfloat16), gated], axis=0)
        filtered = jnp.zeros((TOKENS, S), jnp.float32)
        for tap_index in range(TAPS):
            filtered = filtered + conv_taps[layer_index, tap_index] * padded[tap_index:tap_index + TOKENS].astype(jnp.float32)
        mixed_raw = stored(outer.astype(jnp.float32) * filtered)
        mixed = stored(rms_norm(mixed_raw.astype(jnp.float32), mix_gain[layer_index]))
        branch = stored(jnp.dot(mixed, out_weight[layer_index], preferred_element_type=jnp.float32))
        stream = stream + rms_norm(branch.astype(jnp.float32), post_gain[layer_index])
    return stream.astype(jnp.bfloat16)
```

```python
import functools

import jax
import jax.numpy as jnp
from jax import lax
from jax.experimental import pallas as pl
from jax.experimental.pallas import tpu as pltpu
from jax.sharding import PartitionSpec as P

EPS = 1e-06


def passed_along(x, axis, by):
    length = lax.axis_size(axis)
    pairs = [(i, i + by) for i in range(length) if 0 <= i + by < length]
    return lax.ppermute(x, axis, pairs)


def rms_norm(values, gain):
    return values * lax.rsqrt(jnp.mean(values * values, axis=-1, keepdims=True) + EPS) * gain


def stored(values):
    return lax.optimization_barrier(values.astype(jnp.bfloat16))


def per_device(
    tokens, gate_in, gate_conv, value_in, out_weight, conv_taps, pre_gain, mix_gain, post_gain
):
    layer_count = gate_in.shape[0]
    channel_count = gate_in.shape[2]
    tap_count = conv_taps.shape[1]
    row_count = tokens.shape[0]
    tp_size = lax.axis_size("tp")
    tp_index = lax.axis_index("tp")
    row_share = row_count // tp_size
    stream = tokens.astype(jnp.float32)
    for layer_index in range(layer_count):
        is_last = layer_index == layer_count - 1
        normed = stored(rms_norm(stream, pre_gain[layer_index]))
        outer_whole, inner_whole, value_whole = (
            lax.all_gather(gate_in[layer_index], "sp", axis=0, tiled=True),
            lax.all_gather(gate_conv[layer_index], "sp", axis=0, tiled=True),
            lax.all_gather(value_in[layer_index], "sp", axis=0, tiled=True),
        )
        out_whole = lax.all_gather(out_weight[layer_index], "sp", axis=1, tiled=True)
        outer = stored(jnp.dot(normed, outer_whole, preferred_element_type=jnp.float32))
        inner = stored(jnp.dot(normed, inner_whole, preferred_element_type=jnp.float32))
        values = stored(jnp.dot(normed, value_whole, preferred_element_type=jnp.float32))
        gated = stored(inner.astype(jnp.float32) * values.astype(jnp.float32))
        before = passed_along(gated[row_count - (tap_count - 1) :], "sp", 1)
        padded = jnp.concatenate([before, gated], axis=0)
        taps_here = lax.dynamic_slice_in_dim(
            conv_taps[layer_index], tp_index * channel_count, channel_count, 1
        )
        filtered = jnp.zeros((row_count, channel_count), jnp.float32)
        for tap_index in range(tap_count):
            filtered = filtered + taps_here[tap_index] * padded[
                tap_index : tap_index + row_count
            ].astype(jnp.float32)
        mixed_raw = stored(outer.astype(jnp.float32) * filtered)
        if is_last:
            arrived = lax.all_to_all(mixed_raw, "tp", split_axis=0, concat_axis=1, tiled=True)
            residual = lax.dynamic_slice_in_dim(stream, tp_index * row_share, row_share, 0)
        else:
            arrived = lax.all_gather(mixed_raw, "tp", axis=1, tiled=True)
            residual = stream
        mixed = stored(rms_norm(arrived.astype(jnp.float32), mix_gain[layer_index]))
        branch = stored(jnp.dot(mixed, out_whole, preferred_element_type=jnp.float32))
        stream = residual + rms_norm(branch.astype(jnp.float32), post_gain[layer_index])
    return stream.astype(jnp.bfloat16)


MESH = pl.DeviceIdType.MESH


def fused_kernel(
    sizes,
    tok_hbm, gate_hbm, conv_hbm, value_hbm, outw_hbm, taps_hbm, pre_hbm, mixg_hbm, post_hbm,
    out_ref, taps_ref, pre_ref, mixg_ref, post_ref,
    tok, nrm, w, ow, gpad, outer, halo_tx, halo_rx, m, ms, mlast, mx, br, res,
    loc, zsw, zrw, zso, zro, ysw, yrw, yso, yro, xso, xro, cso, cro, hs, hr_sem, ts, tr, a2s, a2r, small,
):
    layers, grp, sp, tp, ch, rows, depth, cols = sizes
    width = sp * cols
    taps = taps_ref.shape[0]
    g = lax.axis_index("grp")
    s = lax.axis_index("sp")
    t = lax.axis_index("tp")
    x = t // 2
    c = t % 2
    sibling = x * 2 + (1 - c)
    across = (1 - x) * 2 + c
    diagonal = (1 - x) * 2 + (1 - c)
    share = rows // tp
    half = depth // 2
    part = (tp * ch) // (2 * tp)
    pending = []

    def when(cond, body):
        if cond is None:
            body()
        else:
            pl.when(cond)(body)

    def copy(ref_from, ref_to, send, recv, **device):
        return pltpu.make_async_remote_copy(
            src_ref=ref_from, dst_ref=ref_to, send_sem=send, recv_sem=recv,
            device_id=device, device_id_type=MESH,
        )

    def start(cond, make):
        when(cond, lambda: make().start())
        pending.append((cond, make))

    piece_rows = half // PIECES

    def w_half(l, j, h, p):
        first = pl.multiple_of(h * half + p * piece_rows, piece_rows)
        return w.at[l, j, pl.ds(first, piece_rows), :]

    def o_rows(l, j, first, count):
        return ow.at[l, j, pl.ds(pl.multiple_of(first, part), count), :]

    my_part = ((c * 2 + x) * 2 + g) * part
    your_part = ((c * 2 + x) * 2 + (1 - g)) * part

    def z_w(l, j, way, p):
        r = w_half(l, j, g, p)
        return copy(r, r, zsw.at[l, (way + 1) // 2, j, p], zrw.at[l, j, p], sp=s + way)

    def z_o(l, j, way):
        r = o_rows(l, j, my_part, part)
        return copy(r, r, zso.at[l, (way + 1) // 2, j], zro.at[l, j], sp=s + way)

    def y_w(l, j, h, p):
        r = w_half(l, j, h, p)
        return copy(r, r, ysw.at[l, j, p], yrw.at[l, j, p], grp=1 - g)

    def y_o(l, j, first):
        r = o_rows(l, j, first, part)
        return copy(r, r, yso.at[l, j], yro.at[l, j], grp=1 - g)

    def x_o(l, j, side):
        r = o_rows(l, j, (c * 2 + side) * 2 * part, 2 * part)
        return copy(r, r, xso.at[l, j], xro.at[l, j], tp=across)

    def c_o(l, j, core):
        r = o_rows(l, j, core * 4 * part, 4 * part)
        return copy(r, r, cso.at[l, j], cro.at[l, j], tp=sibling)

    def sides(k):
        return ((s >= k, s - k, 1, s < sp - 1), (s + k < sp, s + k, -1, s > 0))

    def both(*conds):
        value = conds[0]
        for cond in conds[1:]:
            value = jnp.logical_and(value, cond)
        return value

    def own_to(l, way, cond):
        for p in range(PIECES):
            start(cond, lambda p=p: z_w(l, s, way, p))
        start(cond, lambda: z_o(l, s, way))

    def own_after(l, k):
        if l >= layers:
            return
        if k == 0:
            when(None, lambda: wait_local(l))
        own_to(l, 1, both(s == k, s < sp - 1))
        own_to(l, -1, both(sp - 1 - s == k, s > 0))

    def fwd(l, k):
        for has, j, way, more in sides(k):
            cond = both(has, more)
            for p in range(PIECES):
                when(cond, lambda: z_w(l, j, way, p).wait_recv())
                start(cond, lambda l=l, j=j, way=way, p=p: z_w(l, j, way, p))
                start(cond, lambda l=l, j=j, p=p: y_w(l, j, g, p))
            when(cond, lambda: z_o(l, j, way).wait_recv())
            start(cond, lambda l=l, j=j, way=way: z_o(l, j, way))
            start(cond, lambda l=l, j=j: y_o(l, j, my_part))

    def end_w(l, k):
        for has, j, way, more in sides(k):
            cond = both(has, jnp.logical_not(more))
            for p in range(PIECES):
                when(cond, lambda: z_w(l, j, way, p).wait_recv())
                start(cond, lambda l=l, j=j, p=p: y_w(l, j, g, p))

    def end_o(l, k):
        for has, j, way, more in sides(k):
            cond = both(has, jnp.logical_not(more))
            when(cond, lambda: z_o(l, j, way).wait_recv())
            start(cond, lambda l=l, j=j: y_o(l, j, my_part))

    def y_wait(l, k):
        for has, j, _, _ in sides(k):
            for p in range(PIECES):
                when(has, lambda: y_w(l, j, 1 - g, p).wait_recv())

    def x_phase(l, k):
        for has, j, _, _ in sides(k):
            when(has, lambda: y_o(l, j, your_part).wait_recv())
            start(has, lambda l=l, j=j: x_o(l, j, x))

    def c_phase(l, k):
        for has, j, _, _ in sides(k):
            when(has, lambda: x_o(l, j, 1 - x).wait_recv())
            start(has, lambda l=l, j=j: c_o(l, j, c))

    def c_wait(l, k):
        for has, j, _, _ in sides(k):
            when(has, lambda: c_o(l, j, 1 - c).wait_recv())

    def local_weights(l):
        made = [
            pltpu.make_async_copy(src.at[l], w.at[l, s, :, pl.ds(i * ch, ch)], loc.at[l, i])
            for i, src in enumerate((gate_hbm, conv_hbm, value_hbm))
        ]
        return made + [pltpu.make_async_copy(outw_hbm.at[l], ow.at[l, s], loc.at[l, 3])]

    def wait_local(l):
        for one in local_weights(l):
            one.wait()

    tok_copy = pltpu.make_async_copy(tok_hbm, tok, loc.at[layers, 0])
    small_copies = [
        pltpu.make_async_copy(src, dst, small.at[i])
        for i, (src, dst) in enumerate(
            ((taps_hbm, taps_ref), (pre_hbm, pre_ref), (mixg_hbm, mixg_ref), (post_hbm, post_ref))
        )
    ]
    for l in range(layers):
        for one in local_weights(l):
            one.start()
        if l == 0:
            tok_copy.start()
            for one in small_copies:
                one.start()

    barrier = pltpu.get_barrier_semaphore()

    def greet(**device):
        pl.semaphore_signal(barrier, inc=1, device_id=device, device_id_type=MESH)

    pl.when(s > 0)(lambda: greet(sp=s - 1))
    pl.when(s < sp - 1)(lambda: greet(sp=s + 1))
    greet(grp=1 - g)
    greet(tp=sibling)
    greet(tp=across)
    greet(tp=diagonal)
    at_end = jnp.logical_or(s == 0, s == sp - 1)
    pl.semaphore_wait(barrier, jnp.where(at_end, 5, 6))

    wait_local(0)
    own_to(0, 1, s < sp - 1)
    own_to(0, -1, s > 0)
    own_after(1, 0)

    block = VPU_ROWS
    tok_copy.wait()
    for one in small_copies:
        one.wait()

    def first_norm(i, carry):
        at = pl.ds(pl.multiple_of(i * block, block), block)
        v = tok[at, :].astype(jnp.float32)
        scale = lax.rsqrt(jnp.sum(v * v, axis=-1, keepdims=True) * (1.0 / width) + EPS)
        nrm[at, :] = (v * scale * pre_ref[0:1, :]).astype(jnp.bfloat16)
        return carry

    lax.fori_loop(0, rows // block, first_norm, 0)

    for k in range(1, sp):
        fwd(0, k)
        end_w(0, k)
        end_o(0, k)
        own_after(1, k)
        if k > 1:
            x_phase(0, k - 1)

    def halo(l):
        return copy(halo_tx.at[l], halo_rx.at[l], hs.at[l], hr_sem.at[l], sp=s + 1)

    hrows = halo_tx.shape[1]
    big = rows // 2

    for l in range(layers):
        last = l == layers - 1
        if not last:
            fwd(l + 1, 1)
        for k in range(1, sp):
            y_wait(l, k)
        if not last:
            end_w(l + 1, 1)
            end_o(l + 1, 1)
        for piece in reversed(range(rows // big)):
            at = pl.ds(piece * big, big)
            prod = jnp.dot(
                nrm[at, :], w[l].reshape(sp * depth, 3 * ch), preferred_element_type=jnp.float32
            ).astype(jnp.bfloat16)
            outer[at, :] = prod[:, :ch]
            gated = (
                prod[:, ch : 2 * ch].astype(jnp.float32) * prod[:, 2 * ch :].astype(jnp.float32)
            ).astype(jnp.bfloat16)
            gpad[pl.ds(8 + piece * big, big), :] = gated.astype(jnp.float32)
            if piece == rows // big - 1:
                halo_tx[l] = gated[big - hrows :, :]
                start(s < sp - 1, lambda l=l: halo(l))
        if last:
            x_phase(l, sp - 1)
        for piece in reversed(range(tp)):
            if piece == 0:
                @pl.when(s == 0)
                def _():
                    gpad[0:8, :] = jnp.zeros((8, ch), jnp.float32)

                @pl.when(s > 0)
                def _():
                    halo(l).wait_recv()
                    gpad[0:8, :] = halo_rx[l].astype(jnp.float32)[hrows - 8 :, :]
            at = pl.ds(piece * share, share)
            filtered = jnp.zeros((share, ch), jnp.float32)
            for k in range(taps):
                tap = taps_ref[k, l : l + 1, pl.ds(pl.multiple_of(t * ch, ch), ch)]
                filtered = filtered + tap * gpad[pl.ds(8 - (taps - 1) + k + piece * share, share), :]
            raw = (outer[at, :].astype(jnp.float32) * filtered).astype(jnp.bfloat16)
            if last:
                ms[at, :] = raw

                @pl.when(t == piece)
                def _():
                    mlast[t] = raw

                start(t != piece, lambda at=at, piece=piece: copy(
                    ms.at[at, :], mlast.at[t], a2s.at[piece], a2r.at[t], tp=piece))
            else:
                m[l, t, at, :] = raw

                def tp_copy(l, j, at, piece, kind, to):
                    r = m.at[l, j, at, :]
                    return copy(r, r, ts.at[l, kind, piece], tr.at[l, j, piece], tp=to)

                start(None, lambda l=l, at=at, piece=piece: tp_copy(l, t, at, piece, 0, across))
                start(None, lambda l=l, at=at, piece=piece: tp_copy(l, t, at, piece, 1, sibling))

        if not last:
            x_phase(l, sp - 1)
            for k in range(2, sp - 1):
                fwd(l + 1, k)
                end_w(l + 1, k)
                end_o(l + 1, k)
            for piece in reversed(range(tp)):
                at = pl.ds(piece * share, share)
                tp_copy(l, across, at, piece, 0, across).wait_recv()
                start(None, lambda l=l, at=at, piece=piece: tp_copy(l, across, at, piece, 2, sibling))
            for k in range(1, sp):
                c_phase(l, k)
            x_phase(l + 1, 1)
            for piece in range(tp):
                at = pl.ds(piece * share, share)
                tp_copy(l, sibling, at, piece, 1, sibling).wait_recv()
                tp_copy(l, diagonal, at, piece, 2, sibling).wait_recv()
        else:
            for k in range(2, sp):
                c_phase(l, k)
            for piece in range(tp):
                @pl.when(t != piece)
                def _():
                    copy(ms.at[pl.ds(0, share), :], mlast.at[piece], a2s.at[piece], a2r.at[piece], tp=piece).wait_recv()

        def mix(read):
            parts = [read(j).astype(jnp.float32) for j in range(tp)]
            total = parts[0] * parts[0]
            for one in parts[1:]:
                total = total + one * one
            scale = lax.rsqrt(jnp.sum(total, axis=-1, keepdims=True) * (1.0 / (tp * ch)) + EPS)
            return [
                (one * scale * mixg_ref[l : l + 1, j * ch : (j + 1) * ch]).astype(jnp.bfloat16)
                for j, one in enumerate(parts)
            ]

        def project(mixed):
            count = mixed.shape[0]
            for j in range(sp):
                br[pl.ds(0, count), j * cols : (j + 1) * cols] = jnp.dot(
                    mixed, ow[l, j], preferred_element_type=jnp.float32
                ).astype(jnp.bfloat16).astype(jnp.float32)

        for k in range(1, sp):
            c_wait(l, k)
        if last:
            mixed = jnp.concatenate(mix(lambda j: mlast[j]), axis=1)
            project(mixed)

            def last_rows(i, carry):
                at = pl.ds(pl.multiple_of(i * block, block), block)
                b = br[at, :]
                scale = lax.rsqrt(jnp.sum(b * b, axis=-1, keepdims=True) * (1.0 / width) + EPS)
                if layers > 1:
                    base = res[at, :]
                else:
                    base = tok[pl.ds(pl.multiple_of(t * share + i * block, block), block), :].astype(jnp.float32)
                out_ref[at, :] = (base + b * scale * post_ref[l : l + 1, :]).astype(jnp.bfloat16)
                return carry

            lax.fori_loop(0, share // block, last_rows, 0)
        else:
            for piece in range(rows // big):
                at = pl.ds(piece * big, big)
                mixed = jnp.concatenate(mix(lambda j: m[l, j, at, :]), axis=1)
                project(mixed)

                def next_rows(i, carry):
                    inside = pl.ds(pl.multiple_of(i * block, block), block)
                    first = piece * big + i * block
                    whole = pl.ds(pl.multiple_of(first, block), block)
                    b = br[inside, :]
                    scale = lax.rsqrt(jnp.sum(b * b, axis=-1, keepdims=True) * (1.0 / width) + EPS)
                    v = tok[whole, :].astype(jnp.float32) + b * scale * post_ref[l : l + 1, :]

                    @pl.when(first // share == t)
                    def _():
                        res[pl.ds(pl.multiple_of(first - t * share, block), block), :] = v

                    scale = lax.rsqrt(jnp.sum(v * v, axis=-1, keepdims=True) * (1.0 / width) + EPS)
                    nrm[whole, :] = (v * scale * pre_ref[l + 1 : l + 2, :]).astype(jnp.bfloat16)
                    return carry

                lax.fori_loop(0, big // block, next_rows, 0)
            end_w(l + 1, sp - 1)
            end_o(l + 1, sp - 1)
            for k in range(2, sp - 1):
                x_phase(l + 1, k)
            c_phase(l + 1, 1)

    for cond, make in pending:
        when(cond, lambda: make().wait_send())


VPU_ROWS = 64
PIECES = 2
VMEM_GRANT = 63 * 1024 * 1024


def fused(sizes, tokens, gate_in, gate_conv, value_in, out_weight, conv_taps, pre_gain, mix_gain, post_gain):
    layers, grp, sp, tp, ch, rows, depth, cols = sizes
    width = sp * cols
    share = rows // tp
    bf, f32 = jnp.bfloat16, jnp.float32
    dma = pltpu.SemaphoreType.DMA
    hbm = pl.BlockSpec(memory_space=pltpu.HBM)
    vmem = pl.BlockSpec(memory_space=pltpu.VMEM)
    taps = jnp.transpose(conv_taps, (1, 0, 2))
    held = pl.pallas_call(
        functools.partial(fused_kernel, sizes),
        out_shape=pltpu.VMEM((share, width), bf),
        in_specs=[hbm] * 9,
        out_specs=vmem,
        scratch_shapes=[
            pltpu.VMEM(taps.shape, f32),
            pltpu.VMEM(pre_gain.shape, f32),
            pltpu.VMEM(mix_gain.shape, f32),
            pltpu.VMEM(post_gain.shape, f32),
            pltpu.VMEM((rows, width), bf),
            pltpu.VMEM((rows, width), bf),
            pltpu.VMEM((layers, sp, depth, 3 * ch), bf),
            pltpu.VMEM((layers, sp, tp * ch, cols), bf),
            pltpu.VMEM((8 + rows, ch), f32),
            pltpu.VMEM((rows, ch), bf),
            pltpu.VMEM((layers, 16, ch), bf),
            pltpu.VMEM((layers, 16, ch), bf),
            pltpu.VMEM((max(layers - 1, 1), tp, rows, ch), bf),
            pltpu.VMEM((rows, ch), bf),
            pltpu.VMEM((tp, share, ch), bf),
            pltpu.VMEM((16, 128), bf),
            pltpu.VMEM((rows // 2, width), f32),
            pltpu.VMEM((share, width), f32),
            dma((layers + 1, 4)),
            dma((layers, 2, sp, PIECES)), dma((layers, sp, PIECES)),
            dma((layers, 2, sp)), dma((layers, sp)),
            dma((layers, sp, PIECES)), dma((layers, sp, PIECES)),
            dma((layers, sp)), dma((layers, sp)),
            dma((layers, sp)), dma((layers, sp)),
            dma((layers, sp)), dma((layers, sp)),
            dma((layers,)), dma((layers,)),
            dma((max(layers - 1, 1), 3, tp)), dma((max(layers - 1, 1), tp, tp)),
            dma((tp,)), dma((tp,)), dma((4,)),
        ],
        compiler_params=pltpu.CompilerParams(
            collective_id=0, has_side_effects=True, vmem_limit_bytes=VMEM_GRANT
        ),
    )(tokens, gate_in, gate_conv, value_in, out_weight, taps, pre_gain, mix_gain, post_gain)
    return held


def fits(sizes, taps):
    layers, grp, sp, tp, ch, rows, depth, cols = sizes
    width = sp * cols
    share = rows // tp
    held = rows * width * 4 + layers * sp * depth * 6 * ch + layers * tp * ch * width * 2
    held += rows * width * 2 + share * width * 8 + layers * tp * rows * ch * 2
    return (
        grp == 2 and tp == 4 and 3 <= sp <= 8 and layers == 2 and taps <= 9
        and ch % 128 == 0 and cols % 128 == 0 and rows % 512 == 0 and depth % 256 == 0
        and held < 40 * 1024 * 1024
    )


def chosen(*arrays):
    tokens, gate_in, _, _, out_weight, conv_taps = arrays[:6]
    sizes = (
        gate_in.shape[0], lax.axis_size("grp"), lax.axis_size("sp"), lax.axis_size("tp"),
        gate_in.shape[2], tokens.shape[0], gate_in.shape[1], out_weight.shape[2],
    )
    if fits(sizes, conv_taps.shape[1]):
        return fused(sizes, *arrays)
    return per_device(*arrays)


def solution(mesh):
    placed = (
        P(("grp", "sp"), None),
        P(None, "sp", "tp"),
        P(None, "sp", "tp"),
        P(None, "sp", "tp"),
        P(None, None, "sp"),
        P(),
        P(),
        P(),
        P(),
    )
    return jax.shard_map(
        chosen,
        mesh=mesh,
        in_specs=placed,
        out_specs=P(("grp", "sp", "tp"), None),
        check_vma=False,
    )
```

```python
import functools

import jax
import jax.numpy as jnp
from jax import lax
from jax.experimental import pallas as pl
from jax.experimental.pallas import tpu as pltpu
from jax.sharding import PartitionSpec as P

EPS = 1e-06


def passed_along(x, axis, by):
    length = lax.axis_size(axis)
    pairs = [(i, i + by) for i in range(length) if 0 <= i + by < length]
    return lax.ppermute(x, axis, pairs)


def rms_norm(values, gain):
    return values * lax.rsqrt(jnp.mean(values * values, axis=-1, keepdims=True) + EPS) * gain


def stored(values):
    return lax.optimization_barrier(values.astype(jnp.bfloat16))


def per_device(
    tokens, gate_in, gate_conv, value_in, out_weight, conv_taps, pre_gain, mix_gain, post_gain
):
    layer_count = gate_in.shape[0]
    channel_count = gate_in.shape[2]
    tap_count = conv_taps.shape[1]
    row_count = tokens.shape[0]
    tp_size = lax.axis_size("tp")
    tp_index = lax.axis_index("tp")
    row_share = row_count // tp_size
    stream = tokens.astype(jnp.float32)
    for layer_index in range(layer_count):
        is_last = layer_index == layer_count - 1
        normed = stored(rms_norm(stream, pre_gain[layer_index]))
        outer_whole, inner_whole, value_whole = (
            lax.all_gather(gate_in[layer_index], "sp", axis=0, tiled=True),
            lax.all_gather(gate_conv[layer_index], "sp", axis=0, tiled=True),
            lax.all_gather(value_in[layer_index], "sp", axis=0, tiled=True),
        )
        out_whole = lax.all_gather(out_weight[layer_index], "sp", axis=1, tiled=True)
        outer = stored(jnp.dot(normed, outer_whole, preferred_element_type=jnp.float32))
        inner = stored(jnp.dot(normed, inner_whole, preferred_element_type=jnp.float32))
        values = stored(jnp.dot(normed, value_whole, preferred_element_type=jnp.float32))
        gated = stored(inner.astype(jnp.float32) * values.astype(jnp.float32))
        before = passed_along(gated[row_count - (tap_count - 1) :], "sp", 1)
        padded = jnp.concatenate([before, gated], axis=0)
        taps_here = lax.dynamic_slice_in_dim(
            conv_taps[layer_index], tp_index * channel_count, channel_count, 1
        )
        filtered = jnp.zeros((row_count, channel_count), jnp.float32)
        for tap_index in range(tap_count):
            filtered = filtered + taps_here[tap_index] * padded[
                tap_index : tap_index + row_count
            ].astype(jnp.float32)
        mixed_raw = stored(outer.astype(jnp.float32) * filtered)
        if is_last:
            arrived = lax.all_to_all(mixed_raw, "tp", split_axis=0, concat_axis=1, tiled=True)
            residual = lax.dynamic_slice_in_dim(stream, tp_index * row_share, row_share, 0)
        else:
            arrived = lax.all_gather(mixed_raw, "tp", axis=1, tiled=True)
            residual = stream
        mixed = stored(rms_norm(arrived.astype(jnp.float32), mix_gain[layer_index]))
        branch = stored(jnp.dot(mixed, out_whole, preferred_element_type=jnp.float32))
        stream = residual + rms_norm(branch.astype(jnp.float32), post_gain[layer_index])
    return stream.astype(jnp.bfloat16)


MESH = pl.DeviceIdType.MESH


def fused_kernel(
    sizes,
    tok_hbm, gate_hbm, conv_hbm, value_hbm, outw_hbm, taps_hbm, pre_hbm, mixg_hbm, post_hbm,
    out_ref, taps_ref, pre_ref, mixg_ref, post_ref,
    tok, nrm, w, ow, gpad, outer, acc, halo_tx, halo_rx, m, ms, mlast, br, res,
    loc, zsw, zrw, zso, zro, ysw, yrw, yso, yro, xsa, xra, xsb, xrb, csa, cra, dso, dro, csb, crb, hs, hr_sem, ts, tr, a2s, a2r, small,
):
    layers, grp, sp, tp, ch, rows, depth, cols = sizes
    width = sp * cols
    taps = taps_ref.shape[0]
    g = lax.axis_index("grp")
    s = lax.axis_index("sp")
    t = lax.axis_index("tp")
    x = t // 2
    c = t % 2
    sibling = x * 2 + (1 - c)
    across = (1 - x) * 2 + c
    diagonal = (1 - x) * 2 + (1 - c)
    share = rows // tp
    half = depth // 2
    part = (tp * ch) // (2 * tp)
    pending = []

    def when(cond, body):
        if cond is None:
            body()
        else:
            pl.when(cond)(body)

    def both(one, other):
        return other if one is None else jnp.logical_and(one, other)

    def copy(ref_from, ref_to, send, recv, **device):
        return pltpu.make_async_remote_copy(
            src_ref=ref_from, dst_ref=ref_to, send_sem=send, recv_sem=recv,
            device_id=device, device_id_type=MESH,
        )

    def start(cond, make):
        when(cond, lambda: make().start())
        pending.append((cond, make))

    def flush(count=None):
        count = len(pending) if count is None else count
        for cond, make in pending[:count]:
            when(cond, lambda: make().wait_send())
        del pending[:count]

    piece_rows = half // PIECES

    def w_half(l, j, h, p):
        first = pl.multiple_of(h * half + p * piece_rows, piece_rows)
        return w.at[l, j, pl.ds(first, piece_rows), :]

    def o_rows(l, j, first, count):
        return ow.at[l, j, pl.ds(pl.multiple_of(first, part), count), :]

    def o_part(side, group):
        return ((c * 2 + side) * 2 + group) * part

    def z_w(l, j, way, p):
        r = w_half(l, j, g, p)
        return copy(r, r, zsw.at[l, (way + 1) // 2, j, p], zrw.at[l, j, p], sp=s + way)

    def z_o(l, j, way):
        r = o_rows(l, j, o_part(x, g), part)
        return copy(r, r, zso.at[l, (way + 1) // 2, j], zro.at[l, j], sp=s + way)

    def y_w(l, j, h, p):
        r = w_half(l, j, h, p)
        return copy(r, r, ysw.at[l, j, p], yrw.at[l, j, p], grp=1 - g)

    def y_o(l, j, group):
        r = o_rows(l, j, o_part(x, group), part)
        return copy(r, r, yso.at[l, j], yro.at[l, j], grp=1 - g)

    def x_a(l, j, side):
        r = o_rows(l, j, o_part(side, g), part)
        return copy(r, r, xsa.at[l, j], xra.at[l, j], tp=across)

    def x_b(l, j, side):
        r = o_rows(l, j, o_part(side, 1 - g), part)
        return copy(r, r, xsb.at[l, j], xrb.at[l, j], tp=across)

    def d_o(side, group):
        l, j = layers - 1, slice_at(sp - 1)
        r = o_rows(l, j, o_part(side, group), part)
        return copy(r, r, dso.at[0], dro.at[0], tp=across, grp=1 - g)

    def c_a(l, j, core):
        r = o_rows(l, j, (core * 2 + x) * 2 * part, 2 * part)
        return copy(r, r, csa.at[l, j], cra.at[l, j], tp=sibling)

    def c_b(l, j, core):
        r = o_rows(l, j, (core * 2 + 1 - x) * 2 * part, 2 * part)
        return copy(r, r, csb.at[l, j], crb.at[l, j], tp=sibling)

    def sides(k):
        return ((s >= k, s - k, 1, s < sp - 1), (s + k < sp, s + k, -1, s > 0))

    below, above = s, sp - 1 - s
    paired = jnp.minimum(below, above)

    def slice_at(i):
        if i == 0:
            return s
        far = (i + 1) // 2
        near = s - far if i % 2 else s + far
        rest = jnp.where(below > above, s - (i - paired), s + (i - paired))
        return jnp.where(i <= 2 * paired, near, rest)

    at_end = jnp.logical_or(s == 0, s == sp - 1)
    inside = jnp.logical_not(at_end)

    def own(l, cond):
        for p in range(PIECES):
            for way, can in ((1, s < sp - 1), (-1, s > 0)):
                start(both(cond, can), lambda way=way, p=p: z_w(l, s, way, p))
        for way, can in ((1, s < sp - 1), (-1, s > 0)):
            start(both(cond, can), lambda way=way: z_o(l, s, way))

    def pump_w(l, k, pieces):
        for p in pieces:
            for has, j, way, more in sides(k):
                when(has, lambda: z_w(l, j, way, p).wait_recv())
                start(both(has, more), lambda l=l, j=j, way=way, p=p: z_w(l, j, way, p))
                start(has, lambda l=l, j=j, p=p: y_w(l, j, g, p))

    def pump_o(l, k):
        for has, j, way, more in sides(k):
            when(has, lambda: z_o(l, j, way).wait_recv())
            start(both(has, more), lambda l=l, j=j, way=way: z_o(l, j, way))
            start(has, lambda l=l, j=j: y_o(l, j, g))
            start(has, lambda l=l, j=j: x_a(l, j, x))
            if l == layers - 1:
                start(both(has, j == slice_at(sp - 1)), lambda: d_o(x, g))

    def pump(l, k):
        pump_w(l, k, range(PIECES))
        pump_o(l, k)

    def direct(l, i):
        return l == layers - 1 and i == sp - 1

    def x_phase(l, i):
        j = slice_at(i)
        y_o(l, j, 1 - g).wait_recv()
        if not direct(l, i):
            start(None, lambda: x_b(l, j, x))
        start(None, lambda: c_a(l, j, c))

    def c_phase(l, i):
        j = slice_at(i)
        x_a(l, j, 1 - x).wait_recv()
        if direct(l, i):
            d_o(1 - x, 1 - g).wait_recv()
        else:
            x_b(l, j, 1 - x).wait_recv()
        start(None, lambda: c_b(l, j, c))

    def c_wait(l, i):
        c_a(l, slice_at(i), 1 - c).wait_recv()
        c_b(l, slice_at(i), 1 - c).wait_recv()

    def local_weights(l):
        made = [
            pltpu.make_async_copy(src.at[l], w.at[l, s, :, pl.ds(i * ch, ch)], loc.at[l, i])
            for i, src in enumerate((gate_hbm, conv_hbm, value_hbm))
        ]
        return made + [pltpu.make_async_copy(outw_hbm.at[l], ow.at[l, s], loc.at[l, 3])]

    def wait_local(l):
        for one in local_weights(l):
            one.wait()

    tok_copy = pltpu.make_async_copy(tok_hbm, tok, loc.at[layers, 0])
    small_copies = [
        pltpu.make_async_copy(src, dst, small.at[i])
        for i, (src, dst) in enumerate(
            ((taps_hbm, taps_ref), (pre_hbm, pre_ref), (mixg_hbm, mixg_ref), (post_hbm, post_ref))
        )
    ]

    barrier = pltpu.get_barrier_semaphore()

    def greet(**device):
        pl.semaphore_signal(barrier, inc=1, device_id=device, device_id_type=MESH)

    pl.when(s > 0)(lambda: greet(sp=s - 1))
    pl.when(s < sp - 1)(lambda: greet(sp=s + 1))
    greet(grp=1 - g)
    greet(tp=sibling)
    greet(tp=across)
    greet(tp=diagonal)
    for l in range(layers):
        for one in local_weights(l):
            one.start()
        if l == 0:
            tok_copy.start()
            for one in small_copies:
                one.start()
    pl.semaphore_wait(barrier, jnp.where(at_end, 5, 6))

    wait_local(0)
    own(0, None)

    block = VPU_ROWS
    big = rows // 2
    tok_copy.wait()
    for one in small_copies:
        one.wait()

    def first_norm(i, carry):
        at = pl.ds(pl.multiple_of(i * block, block), block)
        v = tok[at, :].astype(jnp.float32)
        scale = lax.rsqrt(jnp.sum(v * v, axis=-1, keepdims=True) * (1.0 / width) + EPS)
        nrm[at, :] = (v * scale * pre_ref[0:1, :]).astype(jnp.bfloat16)
        return carry

    def term(l, i, at):
        j = slice_at(i)
        across_depth = pl.ds(pl.multiple_of(j * depth, depth), depth)
        return jnp.dot(nrm[at, across_depth], w[l, j], preferred_element_type=jnp.float32)

    def arrived(l, i):
        j = slice_at(i)
        for p in range(PIECES):
            y_w(l, j, 1 - g, p).wait_recv()

    def add_term(l, i):
        if i > 0:
            arrived(l, i)
        for piece in range(rows // big):
            at = pl.ds(piece * big, big)
            if i == 0:
                acc[at, :] = term(l, i, at)
            else:
                acc[at, :] += term(l, i, at)

    hrows = halo_tx.shape[0]

    def halo():
        return copy(halo_tx, halo_rx, hs.at[0], hr_sem.at[0], sp=s + 1)

    def tail():
        return copy(
            nrm.at[pl.ds(rows - 8, 8), :], nrm.at[pl.ds(rows, 8), :], hs.at[1], hr_sem.at[1], sp=s + 1
        )

    def tail_terms(l):
        pl.when(s > 0)(lambda: tail().wait_recv())
        at = pl.ds(rows, 8)
        total = term(l, 0, at)
        for i in range(1, sp - 1):
            total = total + term(l, i, at)
        acc[at, :] = total

    def last_term(l):
        arrived(l, sp - 1)
        for piece in reversed(range(rows // big)):
            first = piece == rows // big - 1
            extra = 8 if l > 0 and first else 0
            at = pl.ds(piece * big, big + extra)
            prod = (acc[at, :] + term(l, sp - 1, at)).astype(jnp.bfloat16)
            outer[pl.ds(piece * big, big), :] = prod[:big, :ch]
            gated = (
                prod[:, ch : 2 * ch].astype(jnp.float32) * prod[:, 2 * ch :].astype(jnp.float32)
            ).astype(jnp.bfloat16)
            wide = gated.astype(jnp.float32)
            gpad[pl.ds(8 + piece * big, big), :] = wide[:big]
            if extra:
                gpad[0:8, :] = wide[big:]
            elif first:
                halo_tx[...] = gated[big - hrows :, :]
                start(s < sp - 1, halo)

    def fill_halo():
        @pl.when(s == 0)
        def _():
            gpad[0:8, :] = jnp.zeros((8, ch), jnp.float32)

        @pl.when(s > 0)
        def _():
            halo().wait_recv()
            gpad[0:8, :] = halo_rx[...].astype(jnp.float32)[hrows - 8 :, :]

    def convolved(l, piece):
        at = pl.ds(piece * share, share)
        filtered = jnp.zeros((share, ch), jnp.float32)
        for k in range(taps):
            tap = taps_ref[k, l : l + 1, pl.ds(pl.multiple_of(t * ch, ch), ch)]
            filtered = filtered + tap * gpad[pl.ds(8 - (taps - 1) + k + piece * share, share), :]
        return (outer[at, :].astype(jnp.float32) * filtered).astype(jnp.bfloat16)

    def tp_copy(l, j, piece, kind, to):
        r = m.at[l, j, pl.ds(piece * share, share), :]
        return copy(r, r, ts.at[l, kind, piece], tr.at[l, j, piece], tp=to)

    def mix(l, read):
        parts = [read(j).astype(jnp.float32) for j in range(tp)]
        total = parts[0] * parts[0]
        for one in parts[1:]:
            total = total + one * one
        scale = lax.rsqrt(jnp.sum(total, axis=-1, keepdims=True) * (1.0 / (tp * ch)) + EPS)
        return jnp.concatenate([
            (one * scale * mixg_ref[l : l + 1, j * ch : (j + 1) * ch]).astype(jnp.bfloat16)
            for j, one in enumerate(parts)
        ], axis=1)

    def project(l, mixed, j):
        at = pl.ds(j * cols, cols) if isinstance(j, int) else pl.ds(pl.multiple_of(j * cols, cols), cols)
        br[pl.ds(0, mixed.shape[0]), at] = jnp.dot(
            mixed, ow[l, j], preferred_element_type=jnp.float32
        ).astype(jnp.bfloat16).astype(jnp.float32)

    @pl.when(s == 0)
    def _():
        nrm[pl.ds(rows, 8), :] = jnp.zeros((8, width), jnp.bfloat16)

    lax.fori_loop(0, rows // block, first_norm, 0)
    wait_local(1)
    own(1, at_end)
    add_term(0, 0)
    pump(0, 1)
    for k in range(2, sp):
        pump(0, k)
        if k == sp - 2:
            own(1, inside)
        add_term(0, k - 1)
        x_phase(0, k - 1)
        if k > 2:
            c_phase(0, k - 2)

    early = len(pending)
    quarters = [range(n * PIECES // 4, (n + 1) * PIECES // 4) for n in range(4)]
    pump_w(1, 1, quarters[0])
    l = 0
    last_term(l)
    pump_w(1, 1, quarters[1])
    for piece in reversed(range(tp)):
        if piece == 0:
            fill_halo()
        m[l, t, pl.ds(piece * share, share), :] = convolved(l, piece)
        start(None, lambda piece=piece: tp_copy(0, t, piece, 0, across))
        start(None, lambda piece=piece: tp_copy(0, t, piece, 1, sibling))
    pump_w(1, 1, quarters[2])
    x_phase(l, sp - 1)
    c_phase(l, sp - 2)
    pump_w(1, 1, quarters[3])
    for piece in reversed(range(tp)):
        tp_copy(l, across, piece, 0, across).wait_recv()
        start(None, lambda piece=piece: tp_copy(0, across, piece, 2, sibling))
        if piece == tp - 1:
            pump_o(1, 1)
    pump_w(1, 2, quarters[0])
    c_phase(l, sp - 1)
    for i in range(1, sp):
        c_wait(l, i)
    for half_index, piece in enumerate(reversed(range(rows // big))):
        for inner in reversed(range(piece * tp // 2, (piece + 1) * tp // 2)):
            tp_copy(l, sibling, inner, 1, sibling).wait_recv()
            tp_copy(l, diagonal, inner, 2, sibling).wait_recv()
        at = pl.ds(piece * big, big)
        mixed = mix(l, lambda j: m[l, j, at, :])
        for j in range(sp):
            project(l, mixed, j)
            if half_index == 0 and j == sp // 2 - 1:
                pump_w(1, 2, quarters[1])
        if half_index == 0:
            pump_w(1, 2, quarters[2])
        else:
            for k in range(3, sp):
                pump_w(1, k, quarters[0])

        def next_rows(i, carry):
            within = pl.ds(pl.multiple_of(i * block, block), block)
            first = piece * big + i * block
            whole = pl.ds(pl.multiple_of(first, block), block)
            b = br[within, :]
            scale = lax.rsqrt(jnp.sum(b * b, axis=-1, keepdims=True) * (1.0 / width) + EPS)
            v = tok[whole, :].astype(jnp.float32) + b * scale * post_ref[l : l + 1, :]

            @pl.when(first // share == t)
            def _():
                res[pl.ds(pl.multiple_of(first - t * share, block), block), :] = v

            scale = lax.rsqrt(jnp.sum(v * v, axis=-1, keepdims=True) * (1.0 / width) + EPS)
            nrm[whole, :] = (v * scale * pre_ref[l + 1 : l + 2, :]).astype(jnp.bfloat16)
            return carry

        lax.fori_loop(0, big // block, next_rows, 0)
        if half_index == 0:
            start(s < sp - 1, tail)
            pump_w(1, 2, quarters[3])
            pump_o(1, 2)
        else:
            for k in range(3, sp):
                pump_w(1, k, quarters[1])

    l = 1
    add_term(l, 0)
    add_term(l, 1)
    for k in range(3, sp):
        pump_w(1, k, quarters[2])
    x_phase(l, 1)
    for k in range(3, sp):
        add_term(l, k - 1)
        pump_w(1, k, quarters[3])
        x_phase(l, k - 1)
        c_phase(l, k - 2)
        pump_o(1, k)
    tail_terms(l)
    flush(early)
    last_term(l)
    for piece in reversed(range(tp)):
        at = pl.ds(piece * share, share)
        raw = convolved(l, piece)
        ms[at, :] = raw

        @pl.when(t == piece)
        def _():
            mlast[t] = raw

        start(t != piece, lambda at=at, piece=piece: copy(
            ms.at[at, :], mlast.at[t], a2s.at[piece], a2r.at[t], tp=piece))
    c_phase(l, sp - 2)
    x_phase(l, sp - 1)
    c_phase(l, sp - 1)
    for piece in range(tp):
        @pl.when(t != piece)
        def _():
            copy(ms.at[pl.ds(0, share), :], mlast.at[piece], a2s.at[piece], a2r.at[piece], tp=piece).wait_recv()
    mixed = mix(l, lambda j: mlast[j])
    for i in range(sp):
        if i > 0:
            c_wait(l, i)
        project(l, mixed, slice_at(i))

    def last_rows(i, carry):
        at = pl.ds(pl.multiple_of(i * block, block), block)
        b = br[at, :]
        scale = lax.rsqrt(jnp.sum(b * b, axis=-1, keepdims=True) * (1.0 / width) + EPS)
        out_ref[at, :] = (res[at, :] + b * scale * post_ref[l : l + 1, :]).astype(jnp.bfloat16)
        return carry

    lax.fori_loop(0, share // block, last_rows, 0)
    flush()


VPU_ROWS = 64
PIECES = 4
VMEM_GRANT = 63 * 1024 * 1024


def fused(sizes, tokens, gate_in, gate_conv, value_in, out_weight, conv_taps, pre_gain, mix_gain, post_gain):
    layers, grp, sp, tp, ch, rows, depth, cols = sizes
    width = sp * cols
    share = rows // tp
    bf, f32 = jnp.bfloat16, jnp.float32
    dma = pltpu.SemaphoreType.DMA
    hbm = pl.BlockSpec(memory_space=pltpu.HBM)
    vmem = pl.BlockSpec(memory_space=pltpu.VMEM)
    taps = jnp.transpose(conv_taps, (1, 0, 2))
    held = pl.pallas_call(
        functools.partial(fused_kernel, sizes),
        out_shape=pltpu.VMEM((share, width), bf),
        in_specs=[hbm] * 9,
        out_specs=vmem,
        scratch_shapes=[
            pltpu.VMEM(taps.shape, f32),
            pltpu.VMEM(pre_gain.shape, f32),
            pltpu.VMEM(mix_gain.shape, f32),
            pltpu.VMEM(post_gain.shape, f32),
            pltpu.VMEM((rows, width), bf),
            pltpu.VMEM((rows + 8, width), bf),
            pltpu.VMEM((layers, sp, depth, 3 * ch), bf),
            pltpu.VMEM((layers, sp, tp * ch, cols), bf),
            pltpu.VMEM((8 + rows, ch), f32),
            pltpu.VMEM((rows, ch), bf),
            pltpu.VMEM((rows + 8, 3 * ch), f32),
            pltpu.VMEM((16, ch), bf),
            pltpu.VMEM((16, ch), bf),
            pltpu.VMEM((max(layers - 1, 1), tp, rows, ch), bf),
            pltpu.VMEM((rows, ch), bf),
            pltpu.VMEM((tp, share, ch), bf),
            pltpu.VMEM((rows // 2, width), f32),
            pltpu.VMEM((share, width), f32),
            dma((layers + 1, 4)),
            dma((layers, 2, sp, PIECES)), dma((layers, sp, PIECES)),
            dma((layers, 2, sp)), dma((layers, sp)),
            dma((layers, sp, PIECES)), dma((layers, sp, PIECES)),
            dma((layers, sp)), dma((layers, sp)),
            dma((layers, sp)), dma((layers, sp)),
            dma((layers, sp)), dma((layers, sp)),
            dma((layers, sp)), dma((layers, sp)),
            dma((1,)), dma((1,)),
            dma((layers, sp)), dma((layers, sp)),
            dma((2,)), dma((2,)),
            dma((max(layers - 1, 1), 3, tp)), dma((max(layers - 1, 1), tp, tp)),
            dma((tp,)), dma((tp,)), dma((4,)),
        ],
        compiler_params=pltpu.CompilerParams(
            collective_id=0, has_side_effects=True, vmem_limit_bytes=VMEM_GRANT
        ),
    )(tokens, gate_in, gate_conv, value_in, out_weight, taps, pre_gain, mix_gain, post_gain)
    return held


def fits(sizes, taps):
    layers, grp, sp, tp, ch, rows, depth, cols = sizes
    width = sp * cols
    share = rows // tp
    held = rows * width * 4 + layers * sp * depth * 6 * ch + layers * tp * ch * width * 2
    held += rows * width * 2 + share * width * 8 + layers * tp * rows * ch * 2
    return (
        grp == 2 and tp == 4 and 4 <= sp <= 8 and layers == 2 and taps <= 9
        and ch % 128 == 0 and cols % 128 == 0 and rows % 512 == 0 and depth % 256 == 0
        and held < 40 * 1024 * 1024
    )


def chosen(*arrays):
    tokens, gate_in, _, _, out_weight, conv_taps = arrays[:6]
    sizes = (
        gate_in.shape[0], lax.axis_size("grp"), lax.axis_size("sp"), lax.axis_size("tp"),
        gate_in.shape[2], tokens.shape[0], gate_in.shape[1], out_weight.shape[2],
    )
    if fits(sizes, conv_taps.shape[1]):
        return fused(sizes, *arrays)
    return per_device(*arrays)


def solution(mesh):
    placed = (
        P(("grp", "sp"), None),
        P(None, "sp", "tp"),
        P(None, "sp", "tp"),
        P(None, "sp", "tp"),
        P(None, None, "sp"),
        P(),
        P(),
        P(),
        P(),
    )
    return jax.shard_map(
        chosen,
        mesh=mesh,
        in_specs=placed,
        out_specs=P(("grp", "sp", "tp"), None),
        check_vma=False,
    )
```

```python
import functools

import jax
import jax.numpy as jnp
from jax import lax
from jax.experimental import pallas as pl
from jax.experimental.pallas import tpu as pltpu
from jax.sharding import PartitionSpec as P

EPS = 1e-06


def passed_along(x, axis, by):
    length = lax.axis_size(axis)
    pairs = [(i, i + by) for i in range(length) if 0 <= i + by < length]
    return lax.ppermute(x, axis, pairs)


def rms_norm(values, gain):
    return values * lax.rsqrt(jnp.mean(values * values, axis=-1, keepdims=True) + EPS) * gain


def stored(values):
    return lax.optimization_barrier(values.astype(jnp.bfloat16))


def per_device(
    tokens, gate_in, gate_conv, value_in, out_weight, conv_taps, pre_gain, mix_gain, post_gain
):
    layer_count = gate_in.shape[0]
    channel_count = gate_in.shape[2]
    tap_count = conv_taps.shape[1]
    row_count = tokens.shape[0]
    tp_size = lax.axis_size("tp")
    tp_index = lax.axis_index("tp")
    row_share = row_count // tp_size
    stream = tokens.astype(jnp.float32)
    for layer_index in range(layer_count):
        is_last = layer_index == layer_count - 1
        normed = stored(rms_norm(stream, pre_gain[layer_index]))
        outer_whole, inner_whole, value_whole = (
            lax.all_gather(gate_in[layer_index], "sp", axis=0, tiled=True),
            lax.all_gather(gate_conv[layer_index], "sp", axis=0, tiled=True),
            lax.all_gather(value_in[layer_index], "sp", axis=0, tiled=True),
        )
        out_whole = lax.all_gather(out_weight[layer_index], "sp", axis=1, tiled=True)
        outer = stored(jnp.dot(normed, outer_whole, preferred_element_type=jnp.float32))
        inner = stored(jnp.dot(normed, inner_whole, preferred_element_type=jnp.float32))
        values = stored(jnp.dot(normed, value_whole, preferred_element_type=jnp.float32))
        gated = stored(inner.astype(jnp.float32) * values.astype(jnp.float32))
        before = passed_along(gated[row_count - (tap_count - 1) :], "sp", 1)
        padded = jnp.concatenate([before, gated], axis=0)
        taps_here = lax.dynamic_slice_in_dim(
            conv_taps[layer_index], tp_index * channel_count, channel_count, 1
        )
        filtered = jnp.zeros((row_count, channel_count), jnp.float32)
        for tap_index in range(tap_count):
            filtered = filtered + taps_here[tap_index] * padded[
                tap_index : tap_index + row_count
            ].astype(jnp.float32)
        mixed_raw = stored(outer.astype(jnp.float32) * filtered)
        if is_last:
            arrived = lax.all_to_all(mixed_raw, "tp", split_axis=0, concat_axis=1, tiled=True)
            residual = lax.dynamic_slice_in_dim(stream, tp_index * row_share, row_share, 0)
        else:
            arrived = lax.all_gather(mixed_raw, "tp", axis=1, tiled=True)
            residual = stream
        mixed = stored(rms_norm(arrived.astype(jnp.float32), mix_gain[layer_index]))
        branch = stored(jnp.dot(mixed, out_whole, preferred_element_type=jnp.float32))
        stream = residual + rms_norm(branch.astype(jnp.float32), post_gain[layer_index])
    return stream.astype(jnp.bfloat16)


MESH = pl.DeviceIdType.MESH


def fused_kernel(
    sizes,
    tok_hbm, gate_hbm, conv_hbm, value_hbm, outw_hbm, taps_hbm, pre_hbm, mixg_hbm, post_hbm,
    out_ref, taps_ref, pre_ref, mixg_ref, post_ref,
    tok, nrm, w, ow, gpad, outer, acc, halo_tx, halo_rx, m, ms, mlast, br, res,
    lw, lo, lt, small, zsw, zrw, zso, zro, ysw, yrw, yso, yro, xs, xr, cs, cr,
    hs, hr_sem, ts, tra, trs, trd, a2s, a2r,
):
    layers, grp, sp, tp, ch, rows, depth, cols = sizes
    width = sp * cols
    taps = taps_ref.shape[0]
    g = lax.axis_index("grp")
    s = lax.axis_index("sp")
    t = lax.axis_index("tp")
    x = t // 2
    c = t % 2
    sibling = x * 2 + (1 - c)
    across = (1 - x) * 2 + c
    diagonal = (1 - x) * 2 + (1 - c)
    share = rows // tp
    half = depth // 2
    part = (tp * ch) // (2 * tp)
    def when(cond, body):
        if cond is None:
            body()
        else:
            pl.when(cond)(body)

    def both(one, other):
        return other if one is None else jnp.logical_and(one, other)

    def copy(ref_from, ref_to, send, recv, **device):
        return pltpu.make_async_remote_copy(
            src_ref=ref_from, dst_ref=ref_to, send_sem=send, recv_sem=recv,
            device_id=device, device_id_type=MESH,
        )

    def start(cond, make):
        when(cond, lambda: make().start())

    piece_rows = half // PIECES

    def w_half(l, j, h, p):
        first = pl.multiple_of(h * half + p * piece_rows, piece_rows)
        return w.at[l, j, pl.ds(first, piece_rows), :]

    def o_rows(l, j, first, count):
        return ow.at[l, j, pl.ds(pl.multiple_of(first * part, part), count * part), :]

    def o_part(side, group):
        return (c * 2 + group) * 2 + side

    def spot(j, at):
        return lax.rem(j - at - 1 + 2 * sp, sp)

    def z_w(l, j, way, p):
        r = w_half(l, j, g, p)
        return copy(r, r, zsw.at[(way + 1) // 2], zrw.at[l, spot(j, s + way), p], sp=s + way)

    def z_w_in(l, j, way, p):
        r = w_half(l, j, g, p)
        return copy(r, r, zsw.at[0], zrw.at[l, spot(j, s), p], sp=s + way)

    def o_first(count):
        return {1: o_part(x, g), 2: o_part(0, g), 4: c * 4}[count]

    def z_o(l, j, way, count):
        r = o_rows(l, j, o_first(count), count)
        return copy(r, r, zso.at[l, (way + 1) // 2], zro.at[l, spot(j, s + way)], sp=s + way)

    def z_o_in(l, j, way, count):
        r = o_rows(l, j, o_first(count), count)
        return copy(r, r, zso.at[l, 0], zro.at[l, spot(j, s)], sp=s + way)

    def y_w(l, j, p):
        r = w_half(l, j, g, p)
        return copy(r, r, ysw.at[0], yrw.at[l, spot(j, s)], grp=1 - g)

    def y_w_in(l, j):
        r = w.at[l, j, pl.ds(pl.multiple_of((1 - g) * half, half), half), :]
        return copy(r, r, ysw.at[0], yrw.at[l, spot(j, s)], grp=1 - g)

    def y_o(l, j, group, count):
        r = o_rows(l, j, o_part(x if count == 1 else 0, group), count)
        return copy(r, r, yso.at[l], yro.at[l, spot(j, s)], grp=1 - g)

    def x_o(l, j, group):
        r = o_rows(l, j, o_part(x, group), 1)
        return copy(r, r, xs.at[l], xr.at[l, spot(j, s)], tp=across)

    def x_o_in(l, j):
        r = o_rows(l, j, c * 4, 2)
        return copy(r, r, xs.at[l], xr.at[l, spot(j, s)], tp=across)

    def c_o(l, j, core):
        r = o_rows(l, j, core * 4, 4)
        return copy(r, r, cs.at[0], cr.at[spot(j, s) + 1 if l else 0], tp=sibling)

    def c_all(l):
        r = ow.at[l, pl.ds(0, sp - 1), pl.ds(0, 4 * part), :]
        return copy(r, r, cs.at[0], cr.at[0], tp=sibling)

    def sides(k):
        return ((s >= k, s - k, 1, s < sp - 1), (s + k < sp, s + k, -1, s > 0))

    below, above = s, sp - 1 - s
    paired = jnp.minimum(below, above)

    def slice_at(i):
        if i == 0:
            return s
        far = (i + 1) // 2
        near = s - far if i % 2 else s + far
        rest = jnp.where(below > above, s - (i - paired), s + (i - paired))
        return jnp.where(i <= 2 * paired, near, rest)

    at_end = jnp.logical_or(s == 0, s == sp - 1)
    inside = jnp.logical_not(at_end)

    def own(l, cond):
        for p in range(PIECES):
            for way, can in ((1, s < sp - 1), (-1, s > 0)):
                start(both(cond, can), lambda: z_w(l, s, way, p))
        for way, can in ((1, s < sp - 1), (-1, s > 0)):
            if l < layers - 1:
                start(both(cond, can), lambda: z_o(l, s, way, 1))
            else:
                start(both(cond, jnp.logical_and(can, at_end)), lambda: z_o(l, s, way, 4))
                start(both(cond, jnp.logical_and(can, inside)), lambda: z_o(l, s, way, 1))

    def pump_w(l, k, pieces):
        for p in pieces:
            for has, j, way, more in sides(k):
                @pl.when(has)
                def _():
                    z_w_in(l, j, way, p).wait_recv()
                    start(more, lambda: z_w(l, j, way, p))
                    y_w(l, j, p).start()

    def pump_o(l, k, cond=None):
        for has, j, way, more in sides(k):
            first = (s == k) if way == 1 else (s == sp - 1 - k)
            single = has if l < layers - 1 else jnp.logical_and(has, jnp.logical_not(first))

            @pl.when(both(cond, single))
            def _():
                z_o_in(l, j, way, 1).wait_recv()
                start(more, lambda: z_o(l, j, way, 1))
                y_o(l, j, g, 1).start()
                x_o(l, j, g).start()

            if l == layers - 1:
                @pl.when(both(cond, jnp.logical_and(has, first)))
                def _():
                    z_o_in(l, j, way, 4 if k == 1 else 2).wait_recv()
                    start(more, lambda: z_o(l, j, way, 2))
                    if k == 1:
                        c_o(l, j, c).start()
                    else:
                        y_o(l, j, g, 2).start()

    def pump(l, k):
        pump_w(l, k, range(PIECES))
        pump_o(l, k)

    def kind(l, j):
        if l < layers - 1:
            return None, None
        first = jnp.logical_or(j == 0, j == sp - 1)
        near = jnp.logical_or(j == s - 1, j == s + 1)
        return jnp.logical_not(first), jnp.logical_and(first, jnp.logical_not(near))

    def x_phase(l, i):
        j = slice_at(i)
        single, doubled = kind(l, j)

        def relay():
            y_o(l, j, 1 - g, 1).wait_recv()
            x_o(l, j, 1 - g).start()

        def finish():
            y_o(l, j, 1 - g, 2).wait_recv()
            c_o(l, j, c).start()

        when(single, relay)
        if doubled is not None:
            when(doubled, finish)

    def c_phase(l, i):
        j = slice_at(i)
        single, _ = kind(l, j)

        def body():
            x_o_in(l, j).wait_recv()
            c_o(l, j, c).start()

        when(single, body)

    def c_wait(l, i):
        c_o(l, slice_at(i), 1 - c).wait_recv()

    def parts_sent(l, at):
        last = l == layers - 1
        ends = (0, sp - 1)
        others = [j for j in range(sp) if j != at]

        def on_z(j):
            if not last:
                return 1
            return (4 if j in ends else 1) if j == at else (2 if j in ends else 1)

        up = sum(on_z(j) for j in range(at + 1)) if at < sp - 1 else 0
        down = sum(on_z(j) for j in range(at, sp)) if at > 0 else 0
        on_y = sum(1 if not last or j not in ends else 0 if abs(j - at) == 1 else 2 for j in others)
        on_x = sum(2 if not last or j not in ends else 0 for j in others)
        return up, down, on_y, on_x

    def drain():
        def sent(ref, sem, **device):
            copy(ref, ref, sem, a2r.at[0], **device).wait_send()

        def parts(l, count):
            return ow.at[l, 0, pl.ds(0, count * part), :]

        for at in range(sp):
            @pl.when(s == at)
            def _():
                for way, count in ((1, at + 1), (-1, sp - at)):
                    if 0 <= at + way < sp:
                        sent(w.at[:, pl.ds(0, count), pl.ds(0, half), :], zsw.at[(way + 1) // 2], sp=s + way)
                for l in range(layers):
                    up, down, on_y, on_x = parts_sent(l, at)
                    if up:
                        sent(parts(l, up), zso.at[l, 1], sp=s + 1)
                    if down:
                        sent(parts(l, down), zso.at[l, 0], sp=s - 1)
                    sent(parts(l, on_y), yso.at[l], grp=1 - g)
                    if on_x:
                        sent(parts(l, on_x), xs.at[l], tp=across)
        sent(w.at[:, pl.ds(0, sp - 1), pl.ds(0, half), :], ysw.at[0], grp=1 - g)
        sent(ow.at[:, pl.ds(0, sp - 1), pl.ds(0, 4 * part), :], cs.at[0], tp=sibling)
        sent(m.at[0, pl.ds(0, 3)], ts.at[0], tp=sibling)
        sent(mlast.at[pl.ds(0, tp - 1)], a2s.at[0], tp=sibling)

        @pl.when(s < sp - 1)
        def _():
            halo().wait_send()
            tail().wait_send()

    def local_weights(l):
        made = [
            pltpu.make_async_copy(src.at[l], w.at[l, s, :, pl.ds(i * ch, ch)], lw.at[l])
            for i, src in enumerate((gate_hbm, conv_hbm, value_hbm))
        ]
        return made + [pltpu.make_async_copy(outw_hbm.at[l], ow.at[l, s], lo.at[l])]

    def wait_local(l):
        pltpu.make_async_copy(w.at[l, s], w.at[l, s], lw.at[l]).wait()
        pltpu.make_async_copy(outw_hbm.at[l], ow.at[l, s], lo.at[l]).wait()

    tok_copy = pltpu.make_async_copy(tok_hbm, tok, lt.at[0])
    small_copies = [
        pltpu.make_async_copy(src, dst, small.at[i])
        for i, (src, dst) in enumerate(
            ((taps_hbm, taps_ref), (pre_hbm, pre_ref), (mixg_hbm, mixg_ref), (post_hbm, post_ref))
        )
    ]

    barrier = pltpu.get_barrier_semaphore()

    def greet(**device):
        pl.semaphore_signal(barrier, inc=1, device_id=device, device_id_type=MESH)

    pl.when(s > 0)(lambda: greet(sp=s - 1))
    pl.when(s < sp - 1)(lambda: greet(sp=s + 1))
    greet(grp=1 - g)
    greet(tp=sibling)
    greet(tp=across)
    greet(tp=diagonal)
    for l in range(layers):
        for one in local_weights(l):
            one.start()
        if l == 0:
            tok_copy.start()
            for one in small_copies:
                one.start()
    pl.semaphore_wait(barrier, jnp.where(at_end, 5, 6))

    wait_local(0)
    own(0, None)

    block = VPU_ROWS
    big = rows // 2
    tok_copy.wait()
    for one in small_copies:
        one.wait()

    def first_norm(i, carry):
        at = pl.ds(pl.multiple_of(i * block, block), block)
        v = tok[at, :].astype(jnp.float32)
        scale = lax.rsqrt(jnp.sum(v * v, axis=-1, keepdims=True) * (1.0 / width) + EPS)
        nrm[at, :] = (v * scale * pre_ref[0:1, :]).astype(jnp.bfloat16)
        return carry

    def term(l, i, at):
        j = slice_at(i)
        across_depth = pl.ds(pl.multiple_of(j * depth, depth), depth)
        return jnp.dot(nrm[at, across_depth], w[l, j], preferred_element_type=jnp.float32)

    def arrived(l, i):
        y_w_in(l, slice_at(i)).wait_recv()

    def add_term(l, i):
        if i > 0:
            arrived(l, i)
        for piece in range(rows // big):
            at = pl.ds(piece * big, big)
            if i == 0:
                acc[at, :] = term(l, i, at)
            else:
                acc[at, :] += term(l, i, at)

    hrows = halo_tx.shape[0]

    def halo():
        return copy(halo_tx, halo_rx, hs.at[0], hr_sem.at[0], sp=s + 1)

    def tail():
        return copy(
            nrm.at[pl.ds(rows - 8, 8), :], nrm.at[pl.ds(rows, 8), :], hs.at[1], hr_sem.at[1], sp=s + 1
        )

    def tail_terms(l):
        pl.when(s > 0)(lambda: tail().wait_recv())
        at = pl.ds(rows, 8)
        total = term(l, 0, at)
        for i in range(1, sp - 1):
            total = total + term(l, i, at)
        acc[at, :] = total

    def last_term(l):
        arrived(l, sp - 1)
        for piece in reversed(range(rows // big)):
            first = piece == rows // big - 1
            extra = 8 if l > 0 and first else 0
            at = pl.ds(piece * big, big + extra)
            prod = (acc[at, :] + term(l, sp - 1, at)).astype(jnp.bfloat16)
            outer[pl.ds(piece * big, big), :] = prod[:big, :ch]
            gated = (
                prod[:, ch : 2 * ch].astype(jnp.float32) * prod[:, 2 * ch :].astype(jnp.float32)
            ).astype(jnp.bfloat16)
            wide = gated.astype(jnp.float32)
            gpad[pl.ds(8 + piece * big, big), :] = wide[:big]
            if extra:
                gpad[0:8, :] = wide[big:]
            elif first:
                halo_tx[...] = gated[big - hrows :, :]
                start(s < sp - 1, halo)

    def fill_halo():
        @pl.when(s == 0)
        def _():
            gpad[0:8, :] = jnp.zeros((8, ch), jnp.float32)

        @pl.when(s > 0)
        def _():
            halo().wait_recv()
            gpad[0:8, :] = halo_rx[...].astype(jnp.float32)[hrows - 8 :, :]

    def convolved(l, piece):
        at = pl.ds(piece * share, share)
        filtered = jnp.zeros((share, ch), jnp.float32)
        for k in range(taps):
            tap = taps_ref[k, l : l + 1, pl.ds(pl.multiple_of(t * ch, ch), ch)]
            filtered = filtered + tap * gpad[pl.ds(8 - (taps - 1) + k + piece * share, share), :]
        return (outer[at, :].astype(jnp.float32) * filtered).astype(jnp.bfloat16)

    def tp_copy(j, piece, recv, to):
        r = m.at[0, j, pl.ds(piece * share, share), :]
        return copy(r, r, ts.at[0], recv, tp=to)

    def tp_half(j, piece, recv):
        r = m.at[0, j, pl.ds(piece * big, big), :]
        return copy(r, r, ts.at[0], recv.at[piece], tp=sibling)

    def mix(l, read):
        parts = [read(j).astype(jnp.float32) for j in range(tp)]
        total = parts[0] * parts[0]
        for one in parts[1:]:
            total = total + one * one
        scale = lax.rsqrt(jnp.sum(total, axis=-1, keepdims=True) * (1.0 / (tp * ch)) + EPS)
        return jnp.concatenate([
            (one * scale * mixg_ref[l : l + 1, j * ch : (j + 1) * ch]).astype(jnp.bfloat16)
            for j, one in enumerate(parts)
        ], axis=1)

    def project(l, mixed, j):
        at = pl.ds(j * cols, cols) if isinstance(j, int) else pl.ds(pl.multiple_of(j * cols, cols), cols)
        br[pl.ds(0, mixed.shape[0]), at] = jnp.dot(
            mixed, ow[l, j], preferred_element_type=jnp.float32
        ).astype(jnp.bfloat16).astype(jnp.float32)

    @pl.when(s == 0)
    def _():
        nrm[pl.ds(rows, 8), :] = jnp.zeros((8, width), jnp.bfloat16)

    lax.fori_loop(0, rows // block, first_norm, 0)
    wait_local(1)
    own(1, at_end)
    add_term(0, 0)
    pump(0, 1)
    for k in range(2, sp):
        pump(0, k)
        if k == sp - 2:
            own(1, inside)
        add_term(0, k - 1)
        x_phase(0, k - 1)
        if k > 2:
            c_phase(0, k - 2)

    quarters = [range(n * PIECES // 4, (n + 1) * PIECES // 4) for n in range(4)]
    pump_w(1, 1, quarters[0])
    l = 0
    last_term(l)
    pump_w(1, 1, quarters[1])
    for piece in reversed(range(tp)):
        if piece == 0:
            fill_halo()
        m[l, t, pl.ds(piece * share, share), :] = convolved(l, piece)
        tp_copy(t, piece, tra.at[piece], across).start()
        tp_copy(t, piece, trs.at[piece * share // big], sibling).start()
    pump_w(1, 1, quarters[2])
    x_phase(l, sp - 1)
    c_phase(l, sp - 2)
    pump_w(1, 1, quarters[3])
    for piece in reversed(range(tp)):
        tp_copy(across, piece, tra.at[piece], across).wait_recv()
        tp_copy(across, piece, trd.at[piece * share // big], sibling).start()
        if piece == tp - 1:
            pump_o(1, 1)
    pump_w(1, 2, quarters[0])
    c_phase(l, sp - 1)
    c_all(l).wait_recv()
    for half_index, piece in enumerate(reversed(range(rows // big))):
        tp_half(sibling, piece, trs).wait_recv()
        tp_half(diagonal, piece, trd).wait_recv()
        at = pl.ds(piece * big, big)
        mixed = mix(l, lambda j: m[l, j, at, :])
        for j in range(sp):
            project(l, mixed, j)
            if half_index == 0 and j == sp // 2 - 1:
                pump_w(1, 2, quarters[1])
        if half_index == 0:
            pump_w(1, 2, quarters[2])
        else:
            for k in range(3, sp):
                pump_w(1, k, quarters[0])

        def next_rows(i, carry):
            within = pl.ds(pl.multiple_of(i * block, block), block)
            first = piece * big + i * block
            whole = pl.ds(pl.multiple_of(first, block), block)
            b = br[within, :]
            scale = lax.rsqrt(jnp.sum(b * b, axis=-1, keepdims=True) * (1.0 / width) + EPS)
            v = tok[whole, :].astype(jnp.float32) + b * scale * post_ref[l : l + 1, :]

            @pl.when(first // share == t)
            def _():
                res[pl.ds(pl.multiple_of(first - t * share, block), block), :] = v

            scale = lax.rsqrt(jnp.sum(v * v, axis=-1, keepdims=True) * (1.0 / width) + EPS)
            nrm[whole, :] = (v * scale * pre_ref[l + 1 : l + 2, :]).astype(jnp.bfloat16)
            return carry

        lax.fori_loop(0, big // block, next_rows, 0)
        if half_index == 0:
            start(s < sp - 1, tail)
            pump_w(1, 2, quarters[3])
            pump_o(1, 2)
        else:
            for k in range(3, sp):
                pump_w(1, k, quarters[1])

    l = 1
    add_term(l, 0)
    add_term(l, 1)
    for k in range(3, sp):
        pump_w(1, k, quarters[2])
    x_phase(l, 1)
    for k in range(3, sp):
        add_term(l, k - 1)
        pump_w(1, k, quarters[3])
        x_phase(l, k - 1)
        c_phase(l, k - 2)
        pump_o(1, k)
    tail_terms(l)
    last_term(l)
    for piece in reversed(range(tp)):
        at = pl.ds(piece * share, share)
        raw = convolved(l, piece)
        ms[at, :] = raw

        @pl.when(t == piece)
        def _():
            mlast[t] = raw

        start(t != piece, lambda: copy(ms.at[at, :], mlast.at[t], a2s.at[0], a2r.at[0], tp=piece))
    c_phase(l, sp - 2)
    x_phase(l, sp - 1)
    c_phase(l, sp - 1)
    others = mlast.at[pl.ds(0, tp - 1)]
    copy(others, others, a2s.at[0], a2r.at[0], tp=sibling).wait_recv()
    mixed = mix(l, lambda j: mlast[j])
    for i in range(sp):
        if i > 0:
            c_wait(l, i)
        project(l, mixed, slice_at(i))

    def last_rows(i, carry):
        at = pl.ds(pl.multiple_of(i * block, block), block)
        b = br[at, :]
        scale = lax.rsqrt(jnp.sum(b * b, axis=-1, keepdims=True) * (1.0 / width) + EPS)
        out_ref[at, :] = (res[at, :] + b * scale * post_ref[l : l + 1, :]).astype(jnp.bfloat16)
        return carry

    lax.fori_loop(0, share // block, last_rows, 0)
    drain()


VPU_ROWS = 64
PIECES = 4
VMEM_GRANT = 63 * 1024 * 1024


def fused(sizes, tokens, gate_in, gate_conv, value_in, out_weight, conv_taps, pre_gain, mix_gain, post_gain):
    layers, grp, sp, tp, ch, rows, depth, cols = sizes
    width = sp * cols
    share = rows // tp
    bf, f32 = jnp.bfloat16, jnp.float32
    dma = pltpu.SemaphoreType.DMA
    hbm = pl.BlockSpec(memory_space=pltpu.HBM)
    vmem = pl.BlockSpec(memory_space=pltpu.VMEM)
    taps = jnp.transpose(conv_taps, (1, 0, 2))
    held = pl.pallas_call(
        functools.partial(fused_kernel, sizes),
        out_shape=pltpu.VMEM((share, width), bf),
        in_specs=[hbm] * 9,
        out_specs=vmem,
        scratch_shapes=[
            pltpu.VMEM(taps.shape, f32),
            pltpu.VMEM(pre_gain.shape, f32),
            pltpu.VMEM(mix_gain.shape, f32),
            pltpu.VMEM(post_gain.shape, f32),
            pltpu.VMEM((rows, width), bf),
            pltpu.VMEM((rows + 8, width), bf),
            pltpu.VMEM((layers, sp, depth, 3 * ch), bf),
            pltpu.VMEM((layers, sp, tp * ch, cols), bf),
            pltpu.VMEM((8 + rows, ch), f32),
            pltpu.VMEM((rows, ch), bf),
            pltpu.VMEM((rows + 8, 3 * ch), f32),
            pltpu.VMEM((16, ch), bf),
            pltpu.VMEM((16, ch), bf),
            pltpu.VMEM((max(layers - 1, 1), tp, rows, ch), bf),
            pltpu.VMEM((rows, ch), bf),
            pltpu.VMEM((tp, share, ch), bf),
            pltpu.VMEM((rows // 2, width), f32),
            pltpu.VMEM((share, width), f32),
            dma((layers,)), dma((layers,)), dma((1,)), dma((4,)),
            dma((2,)), dma((layers, sp - 1, PIECES)),
            dma((layers, 2)), dma((layers, sp - 1)),
            dma((1,)), dma((layers, sp - 1)),
            dma((layers,)), dma((layers, sp - 1)),
            dma((layers,)), dma((layers, sp - 1)),
            dma((1,)), dma((sp,)),
            dma((2,)), dma((2,)),
            dma((1,)), dma((tp,)), dma((2,)), dma((2,)),
            dma((1,)), dma((1,)),
        ],
        compiler_params=pltpu.CompilerParams(
            collective_id=0, has_side_effects=True, vmem_limit_bytes=VMEM_GRANT
        ),
    )(tokens, gate_in, gate_conv, value_in, out_weight, taps, pre_gain, mix_gain, post_gain)
    return held


def fits(sizes, taps):
    layers, grp, sp, tp, ch, rows, depth, cols = sizes
    width = sp * cols
    share = rows // tp
    held = rows * width * 4 + layers * sp * depth * 6 * ch + layers * tp * ch * width * 2
    held += rows * width * 2 + share * width * 8 + layers * tp * rows * ch * 2
    return (
        grp == 2 and tp == 4 and sp == 4 and layers == 2 and taps <= 9
        and ch % 128 == 0 and cols % 128 == 0 and rows % 512 == 0 and depth % 256 == 0
        and held < 40 * 1024 * 1024
    )


def chosen(*arrays):
    tokens, gate_in, _, _, out_weight, conv_taps = arrays[:6]
    sizes = (
        gate_in.shape[0], lax.axis_size("grp"), lax.axis_size("sp"), lax.axis_size("tp"),
        gate_in.shape[2], tokens.shape[0], gate_in.shape[1], out_weight.shape[2],
    )
    if fits(sizes, conv_taps.shape[1]):
        return fused(sizes, *arrays)
    return per_device(*arrays)


def solution(mesh):
    placed = (
        P(("grp", "sp"), None),
        P(None, "sp", "tp"),
        P(None, "sp", "tp"),
        P(None, "sp", "tp"),
        P(None, None, "sp"),
        P(),
        P(),
        P(),
        P(),
    )
    return jax.shard_map(
        chosen,
        mesh=mesh,
        in_specs=placed,
        out_specs=P(("grp", "sp", "tp"), None),
        check_vma=False,
    )
```

```python
import functools

import jax
import jax.numpy as jnp
from jax import lax
from jax.experimental import pallas as pl
from jax.experimental.pallas import tpu as pltpu
from jax.sharding import PartitionSpec as P

EPS = 1e-06


def passed_along(x, axis, by):
    length = lax.axis_size(axis)
    pairs = [(i, i + by) for i in range(length) if 0 <= i + by < length]
    return lax.ppermute(x, axis, pairs)


def rms_norm(values, gain):
    return values * lax.rsqrt(jnp.mean(values * values, axis=-1, keepdims=True) + EPS) * gain


def stored(values):
    return lax.optimization_barrier(values.astype(jnp.bfloat16))


def per_device(
    tokens, gate_in, gate_conv, value_in, out_weight, conv_taps, pre_gain, mix_gain, post_gain
):
    layer_count = gate_in.shape[0]
    channel_count = gate_in.shape[2]
    tap_count = conv_taps.shape[1]
    row_count = tokens.shape[0]
    tp_size = lax.axis_size("tp")
    tp_index = lax.axis_index("tp")
    row_share = row_count // tp_size
    stream = tokens.astype(jnp.float32)
    for layer_index in range(layer_count):
        is_last = layer_index == layer_count - 1
        normed = stored(rms_norm(stream, pre_gain[layer_index]))
        outer_whole, inner_whole, value_whole = (
            lax.all_gather(gate_in[layer_index], "sp", axis=0, tiled=True),
            lax.all_gather(gate_conv[layer_index], "sp", axis=0, tiled=True),
            lax.all_gather(value_in[layer_index], "sp", axis=0, tiled=True),
        )
        out_whole = lax.all_gather(out_weight[layer_index], "sp", axis=1, tiled=True)
        outer = stored(jnp.dot(normed, outer_whole, preferred_element_type=jnp.float32))
        inner = stored(jnp.dot(normed, inner_whole, preferred_element_type=jnp.float32))
        values = stored(jnp.dot(normed, value_whole, preferred_element_type=jnp.float32))
        gated = stored(inner.astype(jnp.float32) * values.astype(jnp.float32))
        before = passed_along(gated[row_count - (tap_count - 1) :], "sp", 1)
        padded = jnp.concatenate([before, gated], axis=0)
        taps_here = lax.dynamic_slice_in_dim(
            conv_taps[layer_index], tp_index * channel_count, channel_count, 1
        )
        filtered = jnp.zeros((row_count, channel_count), jnp.float32)
        for tap_index in range(tap_count):
            filtered = filtered + taps_here[tap_index] * padded[
                tap_index : tap_index + row_count
            ].astype(jnp.float32)
        mixed_raw = stored(outer.astype(jnp.float32) * filtered)
        if is_last:
            arrived = lax.all_to_all(mixed_raw, "tp", split_axis=0, concat_axis=1, tiled=True)
            residual = lax.dynamic_slice_in_dim(stream, tp_index * row_share, row_share, 0)
        else:
            arrived = lax.all_gather(mixed_raw, "tp", axis=1, tiled=True)
            residual = stream
        mixed = stored(rms_norm(arrived.astype(jnp.float32), mix_gain[layer_index]))
        branch = stored(jnp.dot(mixed, out_whole, preferred_element_type=jnp.float32))
        stream = residual + rms_norm(branch.astype(jnp.float32), post_gain[layer_index])
    return stream.astype(jnp.bfloat16)


MESH = pl.DeviceIdType.MESH


def fused_kernel(
    sizes,
    tok_hbm, gate_hbm, conv_hbm, value_hbm, outw_hbm, taps_hbm, pre_hbm, mixg_hbm, post_hbm,
    out_ref, taps_ref, pre_ref, mixg_ref, post_ref,
    tok, nrm, w, ow, gpad, outer, acc, tail_tx, tail_rx, m, ms, mlast, br, res,
    lw, lo, lt, small, zsw, zrw, zso, zro, ysw, yrw, yso, yro, xs, xr, cs, cr,
    hs, hr_sem, ts, tra, trs, trd, a2s, a2r,
):
    layers, grp, sp, tp, ch, rows, depth, cols = sizes
    width = sp * cols
    taps = taps_ref.shape[0]
    g = lax.axis_index("grp")
    s = lax.axis_index("sp")
    t = lax.axis_index("tp")
    x = t // 2
    c = t % 2
    sibling = x * 2 + (1 - c)
    across = (1 - x) * 2 + c
    diagonal = (1 - x) * 2 + (1 - c)
    share = rows // tp
    half = depth // 2
    part = (tp * ch) // (2 * tp)
    def when(cond, body):
        if cond is None:
            body()
        else:
            pl.when(cond)(body)

    def both(one, other):
        return other if one is None else jnp.logical_and(one, other)

    def copy(ref_from, ref_to, send, recv, **device):
        return pltpu.make_async_remote_copy(
            src_ref=ref_from, dst_ref=ref_to, send_sem=send, recv_sem=recv,
            device_id=device, device_id_type=MESH,
        )

    def start(cond, make):
        when(cond, lambda: make().start())

    piece_rows = half // PIECES

    def w_half(l, j, h, p):
        first = pl.multiple_of(h * half + p * piece_rows, piece_rows)
        return w.at[l, j, pl.ds(first, piece_rows), :]

    def o_rows(l, j, first, count):
        return ow.at[l, j, pl.ds(pl.multiple_of(first * part, part), count * part), :]

    def o_part(side, group):
        return (c * 2 + group) * 2 + side

    def spot(j, at):
        return lax.rem(j - at - 1 + 2 * sp, sp)

    def z_w(l, j, way, p):
        r = w_half(l, j, g, p)
        return copy(r, r, zsw.at[(way + 1) // 2], zrw.at[l, spot(j, s + way), p], sp=s + way)

    def z_w_in(l, j, way, p):
        r = w_half(l, j, g, p)
        return copy(r, r, zsw.at[0], zrw.at[l, spot(j, s), p], sp=s + way)

    def o_piece(l, j, count, q):
        first = {1: o_part(x, g), 2: o_part(0, g), 4: c * 4}[count]
        size = count * part // 2
        return ow.at[l, j, pl.ds(pl.multiple_of(first * part + q * size, size), size), :]

    def z_o(l, j, way, count, q):
        r = o_piece(l, j, count, q)
        return copy(r, r, zso.at[l, (way + 1) // 2], zro.at[l, spot(j, s + way), q], sp=s + way)

    def z_o_in(l, j, way, count, q):
        r = o_piece(l, j, count, q)
        return copy(r, r, zso.at[l, 0], zro.at[l, spot(j, s), q], sp=s + way)

    def y_w(l, j, p):
        r = w_half(l, j, g, p)
        return copy(r, r, ysw.at[0], yrw.at[l, spot(j, s)], grp=1 - g)

    def y_w_in(l, j):
        r = w.at[l, j, pl.ds(pl.multiple_of((1 - g) * half, half), half), :]
        return copy(r, r, ysw.at[0], yrw.at[l, spot(j, s)], grp=1 - g)

    def y_o(l, j, count, q):
        r = o_piece(l, j, count, q)
        return copy(r, r, yso.at[l], yro.at[l, spot(j, s)], grp=1 - g)

    def y_o_in(l, j, count):
        r = o_rows(l, j, o_part(x if count == 1 else 0, 1 - g), count)
        return copy(r, r, yso.at[l], yro.at[l, spot(j, s)], grp=1 - g)

    def x_o(l, j, group):
        r = o_rows(l, j, o_part(x, group), 1)
        return copy(r, r, xs.at[l], xr.at[l, spot(j, s)], tp=across)

    def x_o_in(l, j):
        r = o_rows(l, j, c * 4, 2)
        return copy(r, r, xs.at[l], xr.at[l, spot(j, s)], tp=across)

    def c_o(l, j, core):
        r = o_rows(l, j, core * 4, 4)
        return copy(r, r, cs.at[0], cr.at[spot(j, s) + 1 if l else 0], tp=sibling)

    def c_all(l):
        r = ow.at[l, pl.ds(0, sp - 1), pl.ds(0, 4 * part), :]
        return copy(r, r, cs.at[0], cr.at[0], tp=sibling)

    def sides(k):
        return ((s >= k, s - k, 1, s < sp - 1), (s + k < sp, s + k, -1, s > 0))

    below, above = s, sp - 1 - s
    paired = jnp.minimum(below, above)

    def slice_at(i):
        if i == 0:
            return s
        far = (i + 1) // 2
        near = s - far if i % 2 else s + far
        rest = jnp.where(below > above, s - (i - paired), s + (i - paired))
        return jnp.where(i <= 2 * paired, near, rest)

    at_end = jnp.logical_or(s == 0, s == sp - 1)
    inside = jnp.logical_not(at_end)

    def own(l, cond):
        for p in range(PIECES):
            for way, can in ((1, s < sp - 1), (-1, s > 0)):
                start(both(cond, can), lambda: z_w(l, s, way, p))
        for q in range(2):
            for way, can in ((1, s < sp - 1), (-1, s > 0)):
                if l < layers - 1:
                    start(both(cond, can), lambda: z_o(l, s, way, 1, q))
                else:
                    start(both(cond, jnp.logical_and(can, at_end)), lambda: z_o(l, s, way, 4, q))
                    start(both(cond, jnp.logical_and(can, inside)), lambda: z_o(l, s, way, 1, q))

    def pump_w(l, k, pieces):
        for p in pieces:
            for has, j, way, more in sides(k):
                @pl.when(has)
                def _():
                    z_w_in(l, j, way, p).wait_recv()
                    start(more, lambda: z_w(l, j, way, p))
                    y_w(l, j, p).start()

    def pump_o(l, k, q):
        for has, j, way, more in sides(k):
            first = (s == k) if way == 1 else (s == sp - 1 - k)
            single = has if l < layers - 1 else jnp.logical_and(has, jnp.logical_not(first))

            @pl.when(single)
            def _():
                z_o_in(l, j, way, 1, q).wait_recv()
                start(more, lambda: z_o(l, j, way, 1, q))
                y_o(l, j, 1, q).start()
                if q == 1:
                    x_o(l, j, g).start()

            if l == layers - 1:
                @pl.when(jnp.logical_and(has, first))
                def _():
                    z_o_in(l, j, way, 4 if k == 1 else 2, q).wait_recv()
                    if k > 1:
                        start(more, lambda: z_o(l, j, way, 2, q))
                        y_o(l, j, 2, q).start()
                    elif q == 1:
                        for each in range(2):
                            start(more, lambda: z_o(l, j, way, 2, each))
                        c_o(l, j, c).start()

    def pump(l, k):
        pump_w(l, k, range(PIECES))
        pump_o(l, k, 0)
        pump_o(l, k, 1)

    def pumps(l, k):
        if k >= sp:
            return []
        return [lambda p=p: pump_w(l, k, [p]) for p in range(PIECES)] + [
            lambda q=q: pump_o(l, k, q) for q in range(2)
        ]

    def kind(l, j):
        if l < layers - 1:
            return None, None
        first = jnp.logical_or(j == 0, j == sp - 1)
        near = jnp.logical_or(j == s - 1, j == s + 1)
        return jnp.logical_not(first), jnp.logical_and(first, jnp.logical_not(near))

    def x_phase(l, i):
        j = slice_at(i)
        single, doubled = kind(l, j)

        def relay():
            y_o_in(l, j, 1).wait_recv()
            x_o(l, j, 1 - g).start()

        def finish():
            y_o_in(l, j, 2).wait_recv()
            c_o(l, j, c).start()

        when(single, relay)
        if doubled is not None:
            when(doubled, finish)

    def c_phase(l, i):
        j = slice_at(i)
        single, _ = kind(l, j)

        def body():
            x_o_in(l, j).wait_recv()
            c_o(l, j, c).start()

        when(single, body)

    def c_wait(l, i):
        c_o(l, slice_at(i), 1 - c).wait_recv()

    def parts_sent(l, at):
        last = l == layers - 1
        ends = (0, sp - 1)
        others = [j for j in range(sp) if j != at]

        def on_z(j):
            if not last:
                return 1
            return (4 if j in ends else 1) if j == at else (2 if j in ends else 1)

        up = sum(on_z(j) for j in range(at + 1)) if at < sp - 1 else 0
        down = sum(on_z(j) for j in range(at, sp)) if at > 0 else 0
        on_y = sum(1 if not last or j not in ends else 0 if abs(j - at) == 1 else 2 for j in others)
        on_x = sum(2 if not last or j not in ends else 0 for j in others)
        return up, down, on_y, on_x

    def sent(ref, sem, **device):
        copy(ref, ref, sem, a2r.at[0], **device).wait_send()

    def drain():
        def parts(l, count):
            return ow.at[l, 0, pl.ds(0, count * part), :]

        for at in range(sp):
            @pl.when(s == at)
            def _():
                for way, count in ((1, at + 1), (-1, sp - at)):
                    if 0 <= at + way < sp:
                        sent(w.at[:, pl.ds(0, count), pl.ds(0, half), :], zsw.at[(way + 1) // 2], sp=s + way)
                for l in range(layers):
                    up, down, on_y, on_x = parts_sent(l, at)
                    if up:
                        sent(parts(l, up), zso.at[l, 1], sp=s + 1)
                    if down:
                        sent(parts(l, down), zso.at[l, 0], sp=s - 1)
                    sent(parts(l, on_y), yso.at[l], grp=1 - g)
                    if on_x:
                        sent(parts(l, on_x), xs.at[l], tp=across)
        sent(w.at[:, pl.ds(0, sp - 1), pl.ds(0, half), :], ysw.at[0], grp=1 - g)
        sent(m.at[0, pl.ds(0, 3)], ts.at[0], tp=sibling)

        @pl.when(s < sp - 1)
        def _():
            for l in range(layers):
                tail(l).wait_send()

    def local_weights(l):
        made = [
            pltpu.make_async_copy(src.at[l], w.at[l, s, :, pl.ds(i * ch, ch)], lw.at[l])
            for i, src in enumerate((gate_hbm, conv_hbm, value_hbm))
        ]
        return made + [pltpu.make_async_copy(outw_hbm.at[l], ow.at[l, s], lo.at[l])]

    def wait_local(l):
        pltpu.make_async_copy(w.at[l, s], w.at[l, s], lw.at[l]).wait()
        pltpu.make_async_copy(outw_hbm.at[l], ow.at[l, s], lo.at[l]).wait()

    tok_copy = pltpu.make_async_copy(tok_hbm, tok, lt.at[0])
    small_copies = [
        pltpu.make_async_copy(src, dst, small.at[i])
        for i, (src, dst) in enumerate(
            ((taps_hbm, taps_ref), (pre_hbm, pre_ref), (mixg_hbm, mixg_ref), (post_hbm, post_ref))
        )
    ]

    barrier = pltpu.get_barrier_semaphore()

    def greet(**device):
        pl.semaphore_signal(barrier, inc=1, device_id=device, device_id_type=MESH)

    pl.when(s > 0)(lambda: greet(sp=s - 1))
    pl.when(s < sp - 1)(lambda: greet(sp=s + 1))
    greet(grp=1 - g)
    greet(tp=sibling)
    greet(tp=across)
    greet(tp=diagonal)
    for l in range(layers):
        for one in local_weights(l):
            one.start()
        if l == 0:
            tok_copy.start()
            for one in small_copies:
                one.start()
    pl.semaphore_wait(barrier, jnp.where(at_end, 5, 6))

    wait_local(0)
    own(0, None)

    block = VPU_ROWS
    big = rows // 2
    tok_copy.wait()
    for one in small_copies:
        one.wait()

    def first_norm(i, carry):
        at = pl.ds(pl.multiple_of(i * block, block), block)
        v = tok[at, :].astype(jnp.float32)
        scale = lax.rsqrt(jnp.sum(v * v, axis=-1, keepdims=True) * (1.0 / width) + EPS)
        nrm[at, :] = (v * scale * pre_ref[0:1, :]).astype(jnp.bfloat16)
        return carry

    def term(l, i, at):
        j = slice_at(i)
        across_depth = pl.ds(pl.multiple_of(j * depth, depth), depth)
        return jnp.dot(nrm[at, across_depth], w[l, j], preferred_element_type=jnp.float32)

    def arrived(l, i):
        y_w_in(l, slice_at(i)).wait_recv()

    def add_term(l, i):
        if i > 0:
            arrived(l, i)
        for piece in range(rows // big):
            at = pl.ds(piece * big, big)
            if i == 0:
                acc[at, :] = term(l, i, at)
            else:
                acc[at, :] += term(l, i, at)

    kept = tail_tx.shape[1]

    def tail(l):
        return copy(tail_tx.at[l], tail_rx.at[l], hs.at[l], hr_sem.at[l], sp=s + 1)

    def send_tail(l):
        ending = nrm[pl.ds(rows - 8, 8), :].astype(jnp.float32)
        tail_tx[l] = ending[8 - kept :, :].astype(jnp.bfloat16)
        start(s < sp - 1, lambda: tail(l))

    def tail_terms(l):
        @pl.when(s > 0)
        def _():
            tail(l).wait_recv()
            before = jnp.zeros((8 - kept, width), jnp.float32)
            ending = jnp.concatenate([before, tail_rx[l].astype(jnp.float32)], axis=0)
            nrm[pl.ds(rows, 8), :] = ending.astype(jnp.bfloat16)

        at = pl.ds(rows, 8)
        total = term(l, 0, at)
        for i in range(1, sp - 1):
            total = total + term(l, i, at)
        acc[at, :] = total

    def last_term(l, waiting=()):
        arrived(l, sp - 1)
        for one in waiting:
            one()
        for piece in reversed(range(rows // big)):
            first = piece == rows // big - 1
            extra = 8 if first else 0
            at = pl.ds(piece * big, big + extra)
            prod = (acc[at, :] + term(l, sp - 1, at)).astype(jnp.bfloat16)
            outer[pl.ds(piece * big, big), :] = prod[:big, :ch]
            gated = (
                prod[:, ch : 2 * ch].astype(jnp.float32) * prod[:, 2 * ch :].astype(jnp.float32)
            ).astype(jnp.bfloat16)
            wide = gated.astype(jnp.float32)
            gpad[pl.ds(8 + piece * big, big), :] = wide[:big]
            if extra:
                gpad[0:8, :] = wide[big:]

    def convolved(l, piece):
        at = pl.ds(piece * share, share)
        filtered = jnp.zeros((share, ch), jnp.float32)
        for k in range(taps):
            tap = taps_ref[k, l : l + 1, pl.ds(pl.multiple_of(t * ch, ch), ch)]
            filtered = filtered + tap * gpad[pl.ds(8 - (taps - 1) + k + piece * share, share), :]
        return (outer[at, :].astype(jnp.float32) * filtered).astype(jnp.bfloat16)

    def tp_copy(j, piece, recv, to):
        r = m.at[0, j, pl.ds(piece * share, share), :]
        return copy(r, r, ts.at[0], recv, tp=to)

    def tp_half(j, piece, recv):
        r = m.at[0, j, pl.ds(piece * big, big), :]
        return copy(r, r, ts.at[0], recv.at[piece], tp=sibling)

    def mix(l, read):
        parts = [read(j).astype(jnp.float32) for j in range(tp)]
        total = parts[0] * parts[0]
        for one in parts[1:]:
            total = total + one * one
        scale = lax.rsqrt(jnp.sum(total, axis=-1, keepdims=True) * (1.0 / (tp * ch)) + EPS)
        return jnp.concatenate([
            (one * scale * mixg_ref[l : l + 1, j * ch : (j + 1) * ch]).astype(jnp.bfloat16)
            for j, one in enumerate(parts)
        ], axis=1)

    def project(l, mixed, j):
        at = pl.ds(j * cols, cols) if isinstance(j, int) else pl.ds(pl.multiple_of(j * cols, cols), cols)
        br[pl.ds(0, mixed.shape[0]), at] = jnp.dot(
            mixed, ow[l, j], preferred_element_type=jnp.float32
        ).astype(jnp.bfloat16).astype(jnp.float32)

    @pl.when(s == 0)
    def _():
        nrm[pl.ds(rows, 8), :] = jnp.zeros((8, width), jnp.bfloat16)

    lax.fori_loop(0, rows // block, first_norm, 0)
    send_tail(0)
    wait_local(1)
    own(1, at_end)
    add_term(0, 0)
    pump(0, 1)
    for k in range(2, sp):
        pump(0, k)
        if k == sp - 2:
            own(1, inside)
        add_term(0, k - 1)
        x_phase(0, k - 1)
        if k > 2:
            c_phase(0, k - 2)

    near = pumps(1, 1)
    for one in near[:3]:
        one()
    l = 0
    tail_terms(l)
    last_term(l, near[3:4])

    def send_mixed(piece):
        m[l, t, pl.ds(piece * share, share), :] = convolved(l, piece)
        tp_copy(t, piece, tra.at[piece], across).start()
        tp_copy(t, piece, trs.at[piece * share // big], sibling).start()

    for piece in reversed(range(tp)):
        send_mixed(piece)
    for one in near[4:6]:
        one()
    x_phase(l, sp - 1)
    for one in near[6:8]:
        one()
    c_phase(l, sp - 2)
    mid = pumps(1, 2)
    far = [one for k in range(3, sp) for one in pumps(1, k)]
    between = {3: near[8:10], 2: [], 1: mid[0:2], 0: mid[2:4]}
    for piece in reversed(range(tp)):
        tp_copy(across, piece, tra.at[piece], across).wait_recv()
        tp_copy(across, piece, trd.at[piece * share // big], sibling).start()
        for one in between[piece]:
            one()
    c_phase(l, sp - 1)
    c_all(l).wait_recv()
    steps = iter([
        mid[4:5], mid[5:6], mid[6:8], mid[8:9], mid[9:10],
        [], far[0:2], far[2:3], far[3:4], far[4:6],
    ])

    def advance():
        for one in next(steps):
            one()

    for half_index, piece in enumerate(reversed(range(rows // big))):
        tp_half(sibling, piece, trs).wait_recv()
        tp_half(diagonal, piece, trd).wait_recv()
        advance()
        at = pl.ds(piece * big, big)
        mixed = mix(l, lambda j: m[l, j, at, :])
        for j in range(sp):
            project(l, mixed, j)
            if j % 2:
                advance()

        def next_rows(i, carry):
            within = pl.ds(pl.multiple_of(i * block, block), block)
            first = piece * big + i * block
            whole = pl.ds(pl.multiple_of(first, block), block)
            b = br[within, :]
            scale = lax.rsqrt(jnp.sum(b * b, axis=-1, keepdims=True) * (1.0 / width) + EPS)
            v = tok[whole, :].astype(jnp.float32) + b * scale * post_ref[l : l + 1, :]

            @pl.when(first // share == t)
            def _():
                res[pl.ds(pl.multiple_of(first - t * share, block), block), :] = v

            scale = lax.rsqrt(jnp.sum(v * v, axis=-1, keepdims=True) * (1.0 / width) + EPS)
            nrm[whole, :] = (v * scale * pre_ref[l + 1 : l + 2, :]).astype(jnp.bfloat16)
            return carry

        middle = big // block // 2
        lax.fori_loop(middle, big // block, next_rows, 0)
        if half_index == 0:
            send_tail(1)
        advance()
        lax.fori_loop(0, middle, next_rows, 0)
        advance()

    l = 1
    add_term(l, 0)
    for one in far[6:7]:
        one()
    add_term(l, 1)
    for one in far[7:8]:
        one()
    x_phase(l, 1)
    for k in range(3, sp):
        add_term(l, k - 1)
        for one in far[8:9]:
            one()
        x_phase(l, k - 1)
        for one in far[9:10]:
            one()
    tail_terms(l)
    last_term(l)
    for piece in reversed(range(tp)):
        at = pl.ds(piece * share, share)
        raw = convolved(l, piece)
        ms[at, :] = raw

        @pl.when(t == piece)
        def _():
            mlast[t] = raw

        start(t != piece, lambda: copy(
            ms.at[at, :], mlast.at[t], a2s.at[0], a2r.at[(piece // 2 + x) % 2], tp=piece))
    for i in range(1, sp - 1):
        c_phase(l, i)
    copy(mlast.at[sibling], mlast.at[sibling], a2s.at[0], a2r.at[0], tp=sibling).wait_recv()
    scaled_gain = 2 * ch

    def side_rows(side):
        return pl.ds(pl.multiple_of(side * scaled_gain, scaled_gain), scaled_gain)

    def gained(side):
        gain = mixg_ref[l : l + 1, side_rows(side)]
        both_parts = jnp.concatenate([mlast[2 * side], mlast[2 * side + 1]], axis=1).astype(jnp.float32)
        return both_parts, (both_parts * gain).astype(jnp.bfloat16)

    def columns(i):
        return pl.ds(pl.multiple_of(slice_at(i) * cols, cols), cols)

    def product(mixed, i, side):
        return jnp.dot(mixed, ow[l, slice_at(i), side_rows(side), :], preferred_element_type=jnp.float32)

    mine, mine_mixed = gained(x)
    for i in range(sp - 1):
        if i > 0:
            c_wait(l, i)
        br[pl.ds(0, share), columns(i)] = product(mine_mixed, i, x)
    x_phase(l, sp - 1)
    c_phase(l, sp - 1)
    drain()
    yours_in = mlast.at[pl.ds(0, 2)]
    copy(yours_in, yours_in, a2s.at[0], a2r.at[1], tp=across).wait_recv()
    yours, yours_mixed = gained(1 - x)
    total = jnp.sum(mine * mine + yours * yours, axis=-1, keepdims=True)
    row_scale = lax.rsqrt(total * (1.0 / (tp * ch)) + EPS)
    squares = jnp.zeros((share, 128), jnp.float32)
    for i in range(sp):
        if i < sp - 1:
            sums = br[pl.ds(0, share), columns(i)] + product(yours_mixed, i, 1 - x)
        else:
            c_wait(l, i)
            sums = product(mine_mixed, i, x) + product(yours_mixed, i, 1 - x)
        b = (sums * row_scale).astype(jnp.bfloat16).astype(jnp.float32)
        br[pl.ds(0, share), columns(i)] = b
        for lane in range(0, cols, 128):
            squares = squares + b[:, lane : lane + 128] * b[:, lane : lane + 128]
    scale = lax.rsqrt(jnp.sum(squares, axis=-1, keepdims=True) * (1.0 / width) + EPS)
    out_ref[...] = (res[...] + br[pl.ds(0, share), :] * scale * post_ref[l : l + 1, :]).astype(jnp.bfloat16)
    sent(ow.at[:, pl.ds(0, sp - 1), pl.ds(0, 4 * part), :], cs.at[0], tp=sibling)
    sent(mlast.at[pl.ds(0, tp - 1)], a2s.at[0], tp=sibling)


VPU_ROWS = 64
PIECES = 8
VMEM_GRANT = 63 * 1024 * 1024


def fused(sizes, tokens, gate_in, gate_conv, value_in, out_weight, conv_taps, pre_gain, mix_gain, post_gain):
    layers, grp, sp, tp, ch, rows, depth, cols = sizes
    width = sp * cols
    share = rows // tp
    bf, f32 = jnp.bfloat16, jnp.float32
    dma = pltpu.SemaphoreType.DMA
    hbm = pl.BlockSpec(memory_space=pltpu.HBM)
    vmem = pl.BlockSpec(memory_space=pltpu.VMEM)
    taps = jnp.transpose(conv_taps, (1, 0, 2))
    held = pl.pallas_call(
        functools.partial(fused_kernel, sizes),
        out_shape=pltpu.VMEM((share, width), bf),
        in_specs=[hbm] * 9,
        out_specs=vmem,
        scratch_shapes=[
            pltpu.VMEM(taps.shape, f32),
            pltpu.VMEM(pre_gain.shape, f32),
            pltpu.VMEM(mix_gain.shape, f32),
            pltpu.VMEM(post_gain.shape, f32),
            pltpu.VMEM((rows, width), bf),
            pltpu.VMEM((rows + 8, width), bf),
            pltpu.VMEM((layers, sp, depth, 3 * ch), bf),
            pltpu.VMEM((layers, sp, tp * ch, cols), bf),
            pltpu.VMEM((8 + rows, ch), f32),
            pltpu.VMEM((rows, ch), bf),
            pltpu.VMEM((rows + 8, 3 * ch), f32),
            pltpu.VMEM((layers, taps.shape[0] - 1, width), bf),
            pltpu.VMEM((layers, taps.shape[0] - 1, width), bf),
            pltpu.VMEM((max(layers - 1, 1), tp, rows, ch), bf),
            pltpu.VMEM((rows, ch), bf),
            pltpu.VMEM((tp, share, ch), bf),
            pltpu.VMEM((rows // 2, width), f32),
            pltpu.VMEM((share, width), f32),
            dma((layers,)), dma((layers,)), dma((1,)), dma((4,)),
            dma((2,)), dma((layers, sp - 1, PIECES)),
            dma((layers, 2)), dma((layers, sp - 1, 2)),
            dma((1,)), dma((layers, sp - 1)),
            dma((layers,)), dma((layers, sp - 1)),
            dma((layers,)), dma((layers, sp - 1)),
            dma((1,)), dma((sp,)),
            dma((2,)), dma((2,)),
            dma((1,)), dma((tp,)), dma((2,)), dma((2,)),
            dma((1,)), dma((2,)),
        ],
        compiler_params=pltpu.CompilerParams(
            collective_id=0, has_side_effects=True, vmem_limit_bytes=VMEM_GRANT
        ),
    )(tokens, gate_in, gate_conv, value_in, out_weight, taps, pre_gain, mix_gain, post_gain)
    return held


def fits(sizes, taps):
    layers, grp, sp, tp, ch, rows, depth, cols = sizes
    width = sp * cols
    share = rows // tp
    held = rows * width * 4 + layers * sp * depth * 6 * ch + layers * tp * ch * width * 2
    held += rows * width * 2 + share * width * 8 + layers * tp * rows * ch * 2
    return (
        grp == 2 and tp == 4 and sp == 4 and layers == 2 and taps <= 9
        and ch % 128 == 0 and cols % 128 == 0 and rows % 512 == 0 and depth % 256 == 0
        and held < 40 * 1024 * 1024
    )


def chosen(*arrays):
    tokens, gate_in, _, _, out_weight, conv_taps = arrays[:6]
    sizes = (
        gate_in.shape[0], lax.axis_size("grp"), lax.axis_size("sp"), lax.axis_size("tp"),
        gate_in.shape[2], tokens.shape[0], gate_in.shape[1], out_weight.shape[2],
    )
    if fits(sizes, conv_taps.shape[1]):
        return fused(sizes, *arrays)
    return per_device(*arrays)


def solution(mesh):
    placed = (
        P(("grp", "sp"), None),
        P(None, "sp", "tp"),
        P(None, "sp", "tp"),
        P(None, "sp", "tp"),
        P(None, None, "sp"),
        P(),
        P(),
        P(),
        P(),
    )
    return jax.shard_map(
        chosen,
        mesh=mesh,
        in_specs=placed,
        out_specs=P(("grp", "sp", "tp"), None),
        check_vma=False,
    )
```
